32 devices in a mesh: sp: 4 (over y, x), tp: 8 (over z, core).
Axes of the slice: x: 2, y: 2, z: 4, core: 2. Of those that a mesh axis runs over, the one named last changes fastest.
Arguments:
- query_a: bfloat16 [512, 16, 256], P('sp', 'tp'), may hold values from -5.5 to 5.5
- key_a: bfloat16 [512, 16, 256], P('sp', 'tp'), may hold values from -5.5 to 5.5
- value_a: bfloat16 [512, 16, 256], P('sp', 'tp'), may hold values from -6 to 6
- query_b: bfloat16 [512, 16, 128], P('sp', 'tp'), may hold values from -5.5 to 5.5
- key_b: bfloat16 [512, 16, 128], P('sp', 'tp'), may hold values from -5.5 to 5.5
- value_b: bfloat16 [512, 16, 128], P('sp', 'tp'), may hold values from -6 to 6
- lambdas: float32 [2, 16], P(None, 'tp'), may hold values from 0.3 to 0.8
- gain_a: float32 [256], replicated, may hold values from 0.1 to 1.9
- gain_b: float32 [128], replicated, may hold values from 0.1 to 1.9
- out_a: bfloat16 [4096, 4096], P('tp'), may hold values from -0.078125 to 0.078125
- out_b: bfloat16 [2048, 4096], P('tp'), may hold values from -0.078125 to 0.078125
- residual: bfloat16 [512, 4096], P(('sp', 'tp')), may hold values from -6 to 6
- norm_gain: float32 [4096], replicated, may hold values from 0.1 to 1.9
- route_ids: int32 [512, 2], P(('sp', 'tp')), may hold values from 0 to 7, all different within a row; in each aligned block of 16 rows (0 to 15, 16 to 31, ...) at most 8 rows name the same one
- route_weights: float32 [512, 2], P(('sp', 'tp')), may hold values from 0.1 to 0.9
- w_gate: bfloat16 [8, 4096, 2048], P('sp', None, 'tp'), may hold values from -0.28125 to 0.28125
- w_up: bfloat16 [8, 4096, 2048], P('sp', None, 'tp'), may hold values from -0.28125 to 0.28125
- w_down: bfloat16 [8, 2048, 4096], P('sp', 'tp'), may hold values from -0.01977539 to 0.01977539
Outputs:
- result: bfloat16 [512, 4096], P(('sp', 'tp'))
The draws below stay inside these ranges and needn't reach their ends.
Inputs may be any that keep to these rules, and one draw needn't show every extreme that they name: `route_ids`: in the rows of one device each token names 2 different experts, no expert is named more than 8 times, a bound that some block reaches.
All inputs are finite; a program needn't handle non-finite values.
Results may differ from the reference program's by a relative error of at most 0.02.
Values may be sent and summed in bfloat16 or wider, within the bound.
A program may use at most 128 MiB of HBM per device.

```python
import math
import jax
import jax.numpy as jnp
import numpy as np
from jax import lax

D = 4096
HEADS = 16
DA = 128
DB = 64
VA = 256
VB = 128
F = 2048
TOPK = 2
ROWS = 16
EXPERTS = 8
TOK_DEV = 128
SEQ = 512
CAP = 8
N_SP = 4
N_TP = 8


def paired_maps(key, salt, width):
    base = jax.random.fold_in(key, salt)
    key_query, key_keys = jax.random.split(base, 2)
    shape = (SEQ, HEADS, 2 * width)
    queries = jnp.clip(1.3 * jax.random.normal(key_query, shape, jnp.float32), -5.5, 5.5)
    keys = jnp.clip(1.3 * jax.random.normal(key_keys, shape, jnp.float32), -5.5, 5.5)
    return (queries, keys)


def draw_query_a(key, part):
    return paired_maps(key, 101, DA)[0].astype(jnp.bfloat16)


def draw_key_a(key, part):
    return paired_maps(key, 101, DA)[1].astype(jnp.bfloat16)


def draw_query_b(key, part):
    return paired_maps(key, 202, DB)[0].astype(jnp.bfloat16)


def draw_key_b(key, part):
    return paired_maps(key, 202, DB)[1].astype(jnp.bfloat16)


def shard_levels(own_key, shape, cuts, least, high):
    loudness, own = 1.0, jax.random.fold_in(own_key, 6)
    for dim, blocks in cuts:
        heights = jnp.exp(jax.random.uniform(jax.random.fold_in(own, dim), (blocks,), jnp.float32, least / len(cuts), high / len(cuts)))
        loudness = loudness * jnp.repeat(heights, shape[dim] // blocks).reshape([-1 if axis == dim else 1 for axis in range(len(shape))])
    return loudness


def routed_block(rng, own, number, rows, count, top, bound, lean):
    sequence = jax.random.permutation(rng, count)
    packed, common = shares(count, rows * top, bound, lean, True), shares(count, rows * top, bound, lean, False)
    places = jnp.arange(count)

    def named(sizes, rotation):
        used = int((sizes > 0).sum())
        fixed = max(1, used // 4)
        shifted = fixed + (places - fixed + rotation * (used - fixed)) % max(1, count - fixed)
        return jnp.zeros((count,), jnp.int32).at[sequence[jnp.where(places < fixed, places, shifted)]].set(jnp.asarray(sizes, jnp.int32))

    sizes = jnp.where(number % 4 == 0, named(packed, number // 4), named(common, number - number // 4 - 1))
    mixed = jax.random.permutation(jax.random.fold_in(own, 3), count)
    donor, sink = mixed[0:count // 2 * 2:2], mixed[1:count // 2 * 2:2]
    margin = jnp.minimum(sizes[donor] - 1, bound - sizes[sink]) // 2
    margin = jnp.where((donor == sequence[0]) | (sink == sequence[0]) | (sizes[sink] == 0), 0, jnp.maximum(margin, 0))
    shifted = jax.random.randint(jax.random.fold_in(own, 4), (count // 2,), 0, 1 << 20) % (margin + 1)
    sizes = sizes.at[donor].add(-shifted).at[sink].add(shifted)
    items = jnp.searchsorted(jnp.cumsum(sizes), jnp.arange(rows * top), side="right").astype(jnp.int32)
    grid = items.reshape(top, rows).T
    grid = grid[jax.random.permutation(jax.random.fold_in(own, 1), rows)]
    rotation = jax.random.randint(jax.random.fold_in(own, 2), (rows, 1), 0, top)
    return jnp.take_along_axis(grid, (jnp.arange(top)[None, :] + rotation) % top, axis=1)


def shares(amount, total, limit, skew, full):
    loads = [(1 << 20) // math.isqrt(standing ** skew) + 1 for standing in range(1, amount + 1)]
    largest = limit if full else min(limit, max(-(-total // amount), total * loads[0] // sum(loads)))
    least = 1 if total - largest >= amount - 1 else 0
    given, spare = [largest] + [least] * (amount - 1), total - largest - least * (amount - 1)
    while spare > 0:
        candidates = [i for i in range(1, amount) if given[i] < largest] or [i for i in range(1, amount) if given[i] < limit]
        pool, budget = sum([loads[i] for i in candidates]), spare
        for i in candidates:
            more = min(limit - given[i], max(1, budget * loads[i] // pool), spare)
            given[i] = given[i] + more
            spare = spare - more
    return np.array(given)


def bell_draw(stream_key, dims, scale, most, cuts=(), kind=jnp.bfloat16):
    entries = scale * jax.random.normal(stream_key, dims, jnp.float32)
    if cuts:
        entries = entries * shard_levels(stream_key, dims, cuts, -0.22, 0.18)
    return jnp.clip(entries, -most, most).astype(kind)


def setup_inputs(seed: int = 0) -> dict:
    arg_keys = jax.random.split(jax.random.key(seed), 19)
    query_a = draw_query_a(jax.random.fold_in(arg_keys[18], 71), 0)
    key_a = draw_key_a(jax.random.fold_in(arg_keys[18], 71), 0)
    value_a = bell_draw(arg_keys[2], (SEQ, HEADS, VA), 1.0, 6.0, ((0, 4), (1, 8)))
    query_b = draw_query_b(jax.random.fold_in(arg_keys[18], 71), 0)
    key_b = draw_key_b(jax.random.fold_in(arg_keys[18], 71), 0)
    value_b = bell_draw(arg_keys[5], (SEQ, HEADS, VB), 1.0, 6.0, ((0, 4), (1, 8)))
    lambdas = jnp.clip(0.3 + 0.5 * jax.random.uniform(arg_keys[6], (2, HEADS), jnp.float32) ** shard_levels(arg_keys[6], (2, HEADS), ((1, 8),), -0.2, 0.2), 0.3, 0.8)
    gain_a = jnp.clip(1.0 + 0.18 * jax.random.normal(arg_keys[7], (VA,), jnp.float32), 0.1, 1.9)
    gain_b = jnp.clip(1.0 + 0.18 * jax.random.normal(arg_keys[8], (VB,), jnp.float32), 0.1, 1.9)
    out_a = bell_draw(arg_keys[9], (HEADS * VA, D), (HEADS * (VA + VB)) ** -0.5, 0.078125, ((0, 8),))
    out_b = bell_draw(arg_keys[10], (HEADS * VB, D), (HEADS * (VA + VB)) ** -0.5, 0.078125, ((0, 8),))
    residual = bell_draw(arg_keys[11], (SEQ, D), 1.0, 6.0, ((0, 32),))
    norm_gain = jnp.clip(1.0 + 0.18 * jax.random.normal(arg_keys[12], (D,), jnp.float32), 0.1, 1.9)
    route_ids_keys = jax.random.split(jax.random.fold_in(arg_keys[13], 1), SEQ // ROWS)
    route_ids_turns = jax.random.permutation(jax.random.fold_in(arg_keys[13], 3), SEQ // ROWS)
    route_ids = jax.vmap(lambda own, number: routed_block(jax.random.fold_in(arg_keys[13], 2), own, number, ROWS, EXPERTS, TOPK, CAP, 2))(route_ids_keys, route_ids_turns).reshape((SEQ, TOPK))
    route_weights = jnp.clip(0.1 + 0.79999997 * jax.random.uniform(arg_keys[14], (SEQ, TOPK), jnp.float32) ** shard_levels(arg_keys[14], (SEQ, TOPK), ((0, 32),), -0.2, 0.2), 0.1, 0.9)
    w_gate = bell_draw(arg_keys[15], (EXPERTS, D, F), (3.0 / D ** 0.5), 0.28125, ((0, 4), (2, 8)))
    w_up = bell_draw(arg_keys[16], (EXPERTS, D, F), (3.0 / D ** 0.5), 0.28125, ((0, 4), (2, 8)))
    w_down = bell_draw(arg_keys[17], (EXPERTS, F, D), (0.15 / F ** 0.5), 0.01977539, ((0, 4), (1, 8)))
    return dict(query_a=query_a, key_a=key_a, value_a=value_a, query_b=query_b, key_b=key_b, value_b=value_b, lambdas=lambdas, gain_a=gain_a, gain_b=gain_b, out_a=out_a, out_b=out_b, residual=residual, norm_gain=norm_gain, route_ids=route_ids, route_weights=route_weights, w_gate=w_gate, w_up=w_up, w_down=w_down)


EPSILON = 1e-06
LIMIT = 7.0
SLOPE = 1.702

def head_output(query_head, key_head, value_head, lambda_head, gain, width):
    scaling = width ** (-0.5)

    def block(query_block):
        heard = []
        for which in range(2):
            query_part = query_block[:, which * width:(which + 1) * width]
            key_part = key_head[:, which * width:(which + 1) * width]
            scores = jnp.dot(query_part, key_part.T, preferred_element_type=jnp.float32) * scaling
            highest = lax.optimization_barrier(jnp.max(scores, axis=1, keepdims=True))
            expo = jnp.exp(scores - highest)
            totals = lax.optimization_barrier(jnp.sum(expo, axis=1, keepdims=True))
            summed = jnp.dot(expo.astype(jnp.bfloat16), value_head, preferred_element_type=jnp.float32)
            heard.append(summed / totals)
        differ = heard[0] - lambda_head * heard[1]
        scaled = lax.rsqrt(lax.optimization_barrier(jnp.mean(differ * differ, axis=1, keepdims=True)) + EPSILON)
        return (differ * scaled * gain).astype(jnp.bfloat16)
    blocks = query_head.reshape(SEQ // TOK_DEV, TOK_DEV, 2 * width)
    return lax.map(block, blocks).reshape(SEQ, -1)

def group_output(queries, keys, values, lambda_row, gain, width):

    def one_head(items):
        return head_output(items[0], items[1], items[2], items[3], gain, width)
    heads = lax.map(one_head, (jnp.swapaxes(queries, 0, 1), jnp.swapaxes(keys, 0, 1), jnp.swapaxes(values, 0, 1), lambda_row))
    return jnp.swapaxes(heads, 0, 1).reshape(SEQ, -1)

def reference(query_a, key_a, value_a, query_b, key_b, value_b, lambdas, gain_a, gain_b, out_a, out_b, residual, norm_gain, route_ids, route_weights, w_gate, w_up, w_down):
    attended_a = group_output(query_a, key_a, value_a, lambdas[0], gain_a, DA)
    attended_b = group_output(query_b, key_b, value_b, lambdas[1], gain_b, DB)
    projected = jnp.dot(attended_a, out_a, preferred_element_type=jnp.float32) + jnp.dot(attended_b, out_b, preferred_element_type=jnp.float32)
    mixed = (residual.astype(jnp.float32) + projected).astype(jnp.bfloat16)
    widened = mixed.astype(jnp.float32)
    normed = (widened * lax.rsqrt(lax.optimization_barrier(jnp.mean(widened * widened, axis=1, keepdims=True)) + EPSILON) * norm_gain).astype(jnp.bfloat16)
    hidden_part = F // N_TP
    most_load = N_SP * N_TP * CAP

    def expert_step(running, expert):
        chosen = route_ids == expert
        weight = lax.optimization_barrier(jnp.sum(jnp.where(chosen, route_weights, jnp.float32(0.0)), axis=1))
        marked = jnp.any(chosen, axis=1)
        picked = jnp.nonzero(marked, size=most_load, fill_value=0)[0].astype(jnp.int32)
        counted = jnp.sum(marked.astype(jnp.int32))
        valid = jnp.arange(most_load, dtype=jnp.int32) < counted
        rows = normed[picked]
        gate = jnp.dot(rows, w_gate[expert], preferred_element_type=jnp.float32)
        upward = jnp.dot(rows, w_up[expert], preferred_element_type=jnp.float32)
        clamped = jnp.minimum(gate, LIMIT)
        active = (clamped * jax.nn.sigmoid(SLOPE * clamped) * (jnp.clip(upward, -LIMIT, LIMIT) + 1.0)).astype(jnp.bfloat16)
        blocks = active.astype(jnp.float32).reshape(most_load, N_TP, hidden_part)
        down = w_down[expert].astype(jnp.float32).reshape(N_TP, hidden_part, D)
        partial_value = jnp.einsum('rjf,jfd->jrd', blocks, down).astype(jnp.bfloat16)
        partial_value = lax.optimization_barrier(partial_value)
        expert_out = lax.optimization_barrier(jnp.sum(partial_value.astype(jnp.float32), axis=0)).astype(jnp.bfloat16)
        expert_out = lax.optimization_barrier(expert_out)
        scale_rows = jnp.where(valid, weight[picked], jnp.float32(0.0))
        running = running.at[picked].add(scale_rows[:, None] * expert_out.astype(jnp.float32))
        return (running, None)
    combined, _ = lax.scan(expert_step, jnp.zeros((SEQ, D), jnp.float32), jnp.arange(EXPERTS, dtype=jnp.int32))
    return (widened + combined).astype(jnp.bfloat16)
```

```python
import functools

import jax
import jax.numpy as jnp
from jax import lax
from jax.experimental import pallas as pl
from jax.experimental.pallas import tpu as pltpu
from jax.sharding import PartitionSpec as P

EPSILON = 1e-06
LIMIT = 7.0
SLOPE = 1.702
FLOOR = -1e30


def empty_state(heads_here, queries_here, value_width):
    maxima = jnp.full((2, heads_here, queries_here), FLOOR, jnp.float32)
    totals = jnp.zeros((2, heads_here, queries_here), jnp.float32)
    sums = jnp.zeros((2, heads_here, queries_here, value_width), jnp.float32)
    return (maxima, totals, sums)


def absorb_keys(states, queries, keys, values, width):
    maxima, totals, sums = states
    scaling = width ** (-0.5)
    new_maxima = []
    new_totals = []
    new_sums = []
    for which in range(2):
        query_part = queries[:, :, which * width : (which + 1) * width]
        key_part = keys[:, :, which * width : (which + 1) * width]
        scores = (
            jnp.einsum("qhd,khd->hqk", query_part, key_part, preferred_element_type=jnp.float32)
            * scaling
        )
        highest = jnp.maximum(maxima[which], jnp.max(scores, axis=2))
        expo = jnp.exp(scores - highest[:, :, None])
        factor = jnp.exp(maxima[which] - highest)
        new_totals.append(totals[which] * factor + jnp.sum(expo, axis=2))
        carried = jnp.einsum(
            "hqk,khv->hqv", expo.astype(jnp.bfloat16), values, preferred_element_type=jnp.float32
        )
        new_sums.append(sums[which] * factor[:, :, None] + carried)
        new_maxima.append(highest)
    return (jnp.stack(new_maxima), jnp.stack(new_totals), jnp.stack(new_sums))


def finish(states, lambda_row, gain):
    maxima, totals, sums = states
    heard = sums / totals[:, :, :, None]
    differ = heard[0] - lambda_row[:, None, None] * heard[1]
    scaled = lax.rsqrt(jnp.mean(differ * differ, axis=2, keepdims=True) + EPSILON)
    return (differ * scaled * gain).astype(jnp.bfloat16)


def gated_units(grid, w_gate, w_up):
    gate = jnp.einsum("necd,edf->necf", grid, w_gate, preferred_element_type=jnp.float32)
    upward = jnp.einsum("necd,edf->necf", grid, w_up, preferred_element_type=jnp.float32)
    clamped = jnp.minimum(gate, LIMIT)
    return (
        clamped * jax.nn.sigmoid(SLOPE * clamped) * (jnp.clip(upward, -LIMIT, LIMIT) + 1.0)
    ).astype(jnp.bfloat16)


def per_device_plain(
    query_a,
    key_a,
    value_a,
    query_b,
    key_b,
    value_b,
    lambdas,
    gain_a,
    gain_b,
    out_a,
    out_b,
    residual,
    norm_gain,
    route_ids,
    route_weights,
    w_gate,
    w_up,
    w_down,
):
    heads_here = query_a.shape[1]
    queries_here = query_a.shape[0]
    width_a = query_a.shape[2] // 2
    width_b = query_b.shape[2] // 2
    starting = (
        empty_state(heads_here, queries_here, value_a.shape[2]),
        empty_state(heads_here, queries_here, value_b.shape[2]),
    )
    keys_a = lax.all_gather(key_a, "sp", axis=0, tiled=True)
    values_a = lax.all_gather(value_a, "sp", axis=0, tiled=True)
    keys_b = lax.all_gather(key_b, "sp", axis=0, tiled=True)
    values_b = lax.all_gather(value_b, "sp", axis=0, tiled=True)
    state_a = absorb_keys(starting[0], query_a, keys_a, values_a, width_a)
    state_b = absorb_keys(starting[1], query_b, keys_b, values_b, width_b)
    attended_a = finish(state_a, lambdas[0], gain_a)
    attended_b = finish(state_b, lambdas[1], gain_b)
    model_width = out_a.shape[1]
    weights_a = out_a.reshape(heads_here, -1, model_width)
    weights_b = out_b.reshape(heads_here, -1, model_width)
    first = jnp.einsum("hqv,hvd->qd", attended_a, weights_a, preferred_element_type=jnp.float32)
    projected = lax.psum_scatter(
        (
            first
            + jnp.einsum("hqv,hvd->qd", attended_b, weights_b, preferred_element_type=jnp.float32)
        ).astype(jnp.bfloat16),
        "tp",
        scatter_dimension=0,
        tiled=True,
    ).astype(jnp.float32)
    mixed = (residual.astype(jnp.float32) + projected).astype(jnp.bfloat16)
    widened = mixed.astype(jnp.float32)
    normed = (
        widened
        * lax.rsqrt(jnp.mean(widened * widened, axis=1, keepdims=True) + EPSILON)
        * norm_gain
    ).astype(jnp.bfloat16)
    rows_here, chosen = route_ids.shape
    groups = lax.axis_size("sp")
    experts_here = w_gate.shape[0]
    experts_all = experts_here * groups
    capacity = 2 * rows_here * chosen // experts_all
    slots_here = experts_here * capacity
    flat_ids = route_ids.reshape(-1)
    onehot = (flat_ids[:, None] == jnp.arange(experts_all, dtype=jnp.int32)[None, :]).astype(
        jnp.int32
    )
    earlier = jnp.cumsum(onehot, axis=0) - onehot
    target = flat_ids * capacity + jnp.sum(earlier * onehot, axis=1)
    places = jnp.arange(experts_all * capacity, dtype=jnp.int32)
    layout = jnp.any(target.reshape(rows_here, chosen)[None, :, :] == places[:, None, None], axis=2)
    outgoing = jnp.dot(
        layout.astype(jnp.bfloat16), normed, preferred_element_type=jnp.float32
    ).astype(jnp.bfloat16)
    outgoing = outgoing.reshape(groups, slots_here, model_width)
    arrived = lax.all_to_all(outgoing, "sp", split_axis=0, concat_axis=0, tiled=True)
    pieces = lax.all_gather(arrived, "tp", axis=0, tiled=True)
    count = pieces.shape[0]
    grid = pieces.reshape(count, experts_here, capacity, model_width)
    active = gated_units(grid, w_gate, w_up)
    down = jnp.einsum("necf,efd->necd", active, w_down, preferred_element_type=jnp.float32)
    partial_value = down.astype(jnp.bfloat16).reshape(count, slots_here, model_width)
    totals = lax.psum_scatter(
        partial_value.astype(jnp.float32).astype(jnp.bfloat16),
        "tp",
        scatter_dimension=0,
        tiled=True,
    )
    summed = lax.all_to_all(totals, "sp", split_axis=0, concat_axis=0, tiled=True)
    results = summed.reshape(experts_all * capacity, model_width)
    picked = (
        jnp.take(results, target, axis=0)
        .reshape(rows_here, chosen, model_width)
        .astype(jnp.float32)
    )
    combined = jnp.sum(route_weights[:, :, None] * picked, axis=1)
    return (widened + combined).astype(jnp.bfloat16)


def layer_kernel(
    dims,
    lam_ref,
    ids_ref,
    wts_ref,
    qa_hbm,
    ka_hbm,
    va_hbm,
    qb_hbm,
    kb_hbm,
    vb_hbm,
    gain_a_hbm,
    gain_b_hbm,
    res_hbm,
    norm_hbm,
    out_a_hbm,
    out_b_hbm,
    gate_hbm,
    up_hbm,
    down_hbm,
    o_ref,
    qa_raw,
    ka_raw,
    va_raw,
    qb_raw,
    kb_raw,
    vb_raw,
    gain_a,
    gain_b,
    res,
    norm,
    out_a,
    out_b,
    w_gate,
    w_up,
    w_down,
    spread,
    query_a,
    query_b,
    kv_all,
    att_a,
    att_b,
    acc,
    route,
    part,
    pair1,
    sum1,
    z1,
    tot,
    mixed,
    x_all,
    act,
    contrib,
    pair2,
    red,
    r1,
    mid,
    r2,
    home,
    z2s,
    z2,
    loc_sem,
    kv_s,
    kv_r,
    p1_s,
    p1_r,
    z1_s,
    z1_r,
    gz_s,
    gz_r,
    gs_s,
    gs_r,
    gp_s,
    gp_r,
    p2_s,
    p2_r,
    r1_s,
    r1_r,
    r2_s,
    r2_r,
    z2_s,
    z2_r,
):
    n_sp, n_tp, heads, da, db, va, vb = dims
    nz = n_tp // 2
    f32, bf16 = jnp.float32, jnp.bfloat16
    sp = lax.axis_index("sp")
    tp = lax.axis_index("tp")
    z, core = tp // 2, tp % 2
    rows, width = res.shape
    halves = part.shape[0]
    band = rows // halves
    steps = halves * nz
    chunk = 2 * n_sp * 2 * band
    lanes = route.shape[1]
    wide = width + lanes
    cut = -(-wide // 256) * 128
    side = width // 2
    here = query_a.shape[0]
    experts_here, _, hidden = w_gate.shape
    experts_all = experts_here * n_sp

    x_next = sp + 1 - 2 * (sp % 2)
    y_next = lax.rem(sp + 2, n_sp)
    corner = n_sp - 1 - sp

    def z_at(d):
        return lax.rem(z + d + nz, nz)

    partner = {"sp": sp, "tp": z * 2 + 1 - core}
    to_x = {"sp": x_next, "tp": tp}
    to_y = {"sp": y_next, "tp": tp}

    def to_z(d):
        return {"sp": sp, "tp": z_at(d) * 2 + core}

    def remote(src, dst, send, recv, device):
        return pltpu.make_async_remote_copy(
            src_ref=src,
            dst_ref=dst,
            send_sem=send,
            recv_sem=recv,
            device_id=device,
            device_id_type=pl.DeviceIdType.MESH,
        )

    distant = halves * (nz - 1)

    def step_of(h, d):
        return h * (nz - 1) + d - 1 if d > 0 else distant + h

    def kv_copy(p, i):
        owner, target, half = (
            (sp, to_x, 0),
            (sp, to_y, 1),
            (sp, to_x, 1),
            (sp, to_y, 0),
            (x_next, to_y, 0),
            (y_next, to_x, 1),
        )[i]
        size = here // 2
        place = kv_all.at[p, owner, pl.ds(half * size, size)]
        return remote(place, place, kv_s.at[p, i], kv_r.at[p, i], target)

    def p1_copy(h):
        return remote(part.at[h, 1 - core], pair1.at[h], p1_s.at[h], p1_r.at[h], partner)

    def z1_copy(h, d):
        return remote(
            sum1.at[h, z_at(d)], z1.at[h, d - 1], z1_s.at[h, d - 1], z1_r.at[h, d - 1], to_z(d)
        )

    def gz_copy(h, d):
        return remote(
            x_all.at[step_of(h, 0), sp, core],
            x_all.at[step_of(h, d), sp, core],
            gz_s.at[step_of(h, d)],
            gz_r.at[step_of(h, d)],
            to_z(d),
        )

    def gs_copy(k, i):
        owner, target, half = (
            (sp, to_x, 0),
            (sp, to_y, 1),
            (sp, to_x, 1),
            (sp, to_y, 0),
            (x_next, to_y, 0),
            (y_next, to_x, 1),
        )[i]
        cols = pl.ds(0, cut) if half == 0 else pl.ds(cut, wide - cut)
        place = x_all.at[k, owner, core, :, cols]
        return remote(place, place, gs_s.at[k, i], gs_r.at[k, i], target)

    def gp_copy(k, e):
        block = x_all.at[k, (sp, x_next, y_next, corner)[e], core]
        return remote(block, block, gp_s.at[k, e], gp_r.at[k, e], partner)

    def p2_copy(k):
        return remote(contrib.at[k, 1 - core], pair2.at[k], p2_s.at[k], p2_r.at[k], partner)

    def r1_copy(k, i):
        owner, target, first = (
            (corner, to_x, True),
            (corner, to_y, False),
            (x_next, to_x, True),
            (y_next, to_y, False),
        )[i]
        cols = pl.ds(0, side) if first else pl.ds(side, side)
        return remote(
            red.at[k, owner, :, cols], r1.at[k, i], r1_s.at[k, i], r1_r.at[k, i], target
        )

    def r2_copy(k, i):
        return remote(mid.at[k, i], r2.at[k, i], r2_s.at[k, i], r2_r.at[k, i], (to_y, to_x)[i])

    def z2_copy(k):
        return remote(z2s.at[k], z2.at[k], z2_s.at[k], z2_r.at[k], to_z(-(k % (nz - 1) + 1)))

    moves = (
        (kb_hbm, kb_raw),
        (vb_hbm, vb_raw),
        (ka_hbm, ka_raw),
        (va_hbm, va_raw),
        (qb_hbm, qb_raw),
        (qa_hbm, qa_raw),
        (gain_a_hbm, gain_a),
        (gain_b_hbm, gain_b),
        (out_b_hbm, out_b),
        (out_a_hbm, out_a),
        (res_hbm, res),
        (norm_hbm, norm),
        (gate_hbm, w_gate),
        (up_hbm, w_up),
        (down_hbm, w_down),
    )
    loads = [
        pltpu.make_async_copy(src, dst, loc_sem.at[i]) for i, (src, dst) in enumerate(moves)
    ]
    barrier = pltpu.get_barrier_semaphore()
    greeted = [to_x, to_y, partner] + [to_z(d) for d in range(1, nz)]
    for device in greeted:
        pl.semaphore_signal(
            barrier, inc=1, device_id=device, device_id_type=pl.DeviceIdType.MESH
        )
    for load in loads:
        load.start()

    def deal(raw, out, base, slots):
        count = raw.shape[0]
        spread[:count] = raw[...].astype(f32)
        stride = count // here
        for i in range(stride):
            column = base + slots(i)
            out[:, column : column + 128] = spread[pl.ds(i, here, stride=stride), :].astype(bf16)

    loads[0].wait()
    loads[1].wait()
    own_b = kv_all.at[0, sp]
    deal(kb_raw, own_b, 0, lambda i: i * 128)
    deal(vb_raw, own_b, heads * 2 * db, lambda i: i * 128)
    pl.semaphore_wait(barrier, len(greeted))
    for i in range(4):
        kv_copy(0, i).start()

    def deal_a(raw, base):
        count = raw.shape[0]
        spread[:count] = raw[...].astype(f32)
        stride = count // here
        for i in range(stride):
            c, h = i // heads, i % heads
            column = base + c * 128
            kv_all[1 + h, sp, :, column : column + 128] = spread[
                pl.ds(i, here, stride=stride), :
            ].astype(bf16)

    loads[2].wait()
    deal_a(ka_raw, 0)
    loads[3].wait()
    deal_a(va_raw, 2 * da)
    for i in range(4):
        kv_copy(1, i).start()
    loads[4].wait()
    deal(qb_raw, query_b, 0, lambda i: i * 128)
    loads[5].wait()
    deal(qa_raw, query_a, 0, lambda i: (i % heads) * 2 * da + (i // heads) * 128)
    lane = lax.broadcasted_iota(jnp.int32, (1, lanes), 1)
    folded = jnp.where(lane < experts_all, lane, lane - experts_all)
    for r in range(rows):
        row = jnp.zeros((1, lanes), f32)
        for j in range(ids_ref.shape[0]):
            row += jnp.where(folded == ids_ref[j, r], wts_ref[j, r], 0.0)
        route[r : r + 1, :] = row

    for i in range(2):
        kv_copy(0, i).wait_recv()
        kv_copy(0, 4 + i).start()
    for p in range(2, 1 + heads):
        for i in range(4):
            kv_copy(p, i).start()
    for i in range(2):
        kv_copy(1, i).wait_recv()
        kv_copy(1, 4 + i).start()

    positions = here * n_sp

    def attend(p, q_ref, q0, k0, v0, map_width, value_width, lam, gain):
        heard = []
        for which in range(2):
            if map_width % 128 == 0:
                query = q_ref[:, q0 + which * map_width : q0 + (which + 1) * map_width]
                keys = kv_all[p, :, :, k0 + which * map_width : k0 + (which + 1) * map_width]
            else:
                query = q_ref[:, q0 : q0 + 2 * map_width]
                at = lax.broadcasted_iota(jnp.int32, query.shape, 1)
                inside = (at >= which * map_width) & (at < (which + 1) * map_width)
                query = jnp.where(inside, query.astype(f32), 0.0).astype(bf16)
                keys = kv_all[p, :, :, k0 : k0 + 2 * map_width]
            keys = keys.reshape(positions, keys.shape[2])
            scores = lax.dot_general(
                query, keys, (((1,), (1,)), ((), ())), preferred_element_type=f32
            ) * (map_width**-0.5)
            expo = jnp.exp(scores - jnp.max(scores, axis=1, keepdims=True))
            total = jnp.sum(expo, axis=1, keepdims=True)
            values = kv_all[p, :, :, v0 : v0 + value_width].reshape(positions, value_width)
            carried = jnp.dot(expo.astype(bf16), values, preferred_element_type=f32)
            heard.append(carried / total)
        differ = heard[0] - lam * heard[1]
        scaled = lax.rsqrt(jnp.mean(differ * differ, axis=1, keepdims=True) + EPSILON)
        return (differ * scaled * gain).astype(bf16)

    def attend_a(h):
        att_a[:, h * va : (h + 1) * va] = attend(
            1 + h, query_a, h * 2 * da, 0, 2 * da, da, va, lam_ref[0, h], gain_a[...]
        )

    for load in loads[6:10]:
        load.wait()
    for i in range(2, 6):
        kv_copy(0, i).wait_recv()
    for h in range(heads):
        att_b[:, h * vb : (h + 1) * vb] = attend(
            0,
            query_b,
            h * 2 * db,
            h * 2 * db,
            heads * 2 * db + h * vb,
            db,
            vb,
            lam_ref[1, h],
            gain_b[...],
        )
    for p in range(2, 1 + heads):
        for i in range(2):
            kv_copy(p, i).wait_recv()
            kv_copy(p, 4 + i).start()
    for h in range(heads - 1):
        for i in range(2, 6):
            kv_copy(1 + h, i).wait_recv()
        attend_a(h)
    tile, group = 512, 4
    known = (heads - 1) * va

    @pl.loop(0, width // (tile * group))
    def _(i):
        for g in range(group):
            cols = pl.ds(pl.multiple_of((i * group + g) * tile, tile), tile)
            acc[:, cols] = jnp.dot(
                att_a[:, :known], out_a[:known, cols], preferred_element_type=f32
            ) + jnp.dot(att_b[...], out_b[:, cols], preferred_element_type=f32)

    for i in range(2, 6):
        kv_copy(heads, i).wait_recv()
    attend_a(heads - 1)

    @pl.loop(0, width // (tile * group))
    def _(i):
        for g in range(group):
            cols = pl.ds(pl.multiple_of((i * group + g) * tile, tile), tile)
            value = acc[:, cols] + jnp.dot(
                att_a[:, known:], out_a[known:, cols], preferred_element_type=f32
            )
            value = value.astype(bf16)
            for zz in range(nz):
                for c in range(2):
                    for h in range(halves):
                        r = (zz * 2 + c) * rows + h * band
                        part[h, c, zz, :, cols] = value[r : r + band]

    for h in range(halves):
        p1_copy(h).start()
    loads[10].wait()
    loads[11].wait()

    def fold(h):
        p1_copy(h).wait_recv()
        for d in range(1, nz):
            zz = z_at(d)
            sum1[h, zz] = (part[h, core, zz].astype(f32) + pair1[h, zz].astype(f32)).astype(bf16)
            if h == 0:
                z1_copy(h, d).start()
        tot[h] = part[h, core, z].astype(f32) + pair1[h, z].astype(f32)

    fold(0)
    fold(1)

    def normalise(h):
        total = tot[h]
        for d in range(1, nz):
            z1_copy(h, d).wait_recv()
            total += z1[h, d - 1].astype(f32)
        here_rows = slice(h * band, (h + 1) * band)
        mix = (res[here_rows].astype(f32) + total).astype(bf16)
        mixed[h] = mix
        full = mix.astype(f32)
        scaled = lax.rsqrt(jnp.mean(full * full, axis=1, keepdims=True) + EPSILON)
        x_all[step_of(h, 0), sp, core, :, :width] = (full * scaled * norm[...]).astype(bf16)
        weights = route[here_rows]
        high = weights.astype(bf16).astype(f32)
        at = lax.broadcasted_iota(jnp.int32, weights.shape, 1)
        x_all[step_of(h, 0), sp, core, :, width:] = jnp.where(
            at < experts_all, high, weights - high
        ).astype(bf16)
        for d in range(1, nz):
            gz_copy(h, d).start()

    def arrive(k):
        block = x_all.at[k, sp, core]
        remote(block, block, gz_s.at[k], gz_r.at[k], to_z(1)).wait_recv()

    def open_step(k):
        for i in range(4):
            gs_copy(k, i).start()
        gp_copy(k, 0).start()

    def relay(k):
        for i in range(2):
            gs_copy(k, i).wait_recv()
            gs_copy(k, 4 + i).start()

    def collect(k):
        gs_copy(k, 2).wait_recv()
        gp_copy(k, 1).start()
        gs_copy(k, 3).wait_recv()
        gp_copy(k, 2).start()
        gs_copy(k, 4).wait_recv()
        gs_copy(k, 5).wait_recv()
        gp_copy(k, 3).start()

    def compute(q):
        for i in range(2):
            for e in range(4):
                gp_copy(2 * q + i, e).wait_recv()
        both = pl.ds(2 * q, 2)
        share = x_all[both, :, :, :, width:].reshape(chunk, lanes).astype(f32)
        at = lax.broadcasted_iota(jnp.int32, share.shape, 1)
        x = x_all[both, :, :, :, :width].reshape(chunk, width)
        for j in range(experts_here):
            which = sp * experts_here + j
            weight = jnp.sum(
                jnp.where((at == which) | (at == which + experts_all), share, 0.0),
                axis=1,
                keepdims=True,
            )
            gate = jnp.dot(x, w_gate[j], preferred_element_type=f32)
            upward = jnp.dot(x, w_up[j], preferred_element_type=f32)
            clamped = jnp.minimum(gate, LIMIT)
            active = (
                clamped * jax.nn.sigmoid(SLOPE * clamped) * (jnp.clip(upward, -LIMIT, LIMIT) + 1.0)
            )
            act[:, j * hidden : (j + 1) * hidden] = (active * weight).astype(bf16)

        @pl.loop(0, width // (tile * group))
        def _(i):
            for g in range(group):
                cols = pl.ds(pl.multiple_of((i * group + g) * tile, tile), tile)
                rowsum = jnp.zeros((chunk, tile), f32)
                for j in range(experts_here):
                    rowsum += jnp.dot(
                        act[:, j * hidden : (j + 1) * hidden],
                        w_down[j, :, cols],
                        preferred_element_type=f32,
                    )
                value = rowsum.astype(bf16)
                for t in range(2):
                    for s in range(n_sp):
                        for c in range(2):
                            r = ((t * n_sp + s) * 2 + c) * band
                            contrib[2 * q + t, c, s, :, cols] = value[r : r + band]

        for i in range(2):
            p2_copy(2 * q + i).start()

    first_cols, last_cols = slice(0, side), slice(side, 2 * side)

    def join(k, s, cols):
        red[k, s, :, cols] = (
            contrib[k, core, s, :, cols].astype(f32) + pair2[k, s, :, cols].astype(f32)
        ).astype(bf16)

    def reduce_out(k):
        p2_copy(k).wait_recv()
        join(k, corner, first_cols)
        r1_copy(k, 0).start()
        join(k, corner, last_cols)
        r1_copy(k, 1).start()
        join(k, x_next, first_cols)
        r1_copy(k, 2).start()
        join(k, y_next, last_cols)
        r1_copy(k, 3).start()

    def reduce_mid(k):
        join(k, y_next, first_cols)
        join(k, x_next, last_cols)
        r1_copy(k, 0).wait_recv()
        mid[k, 0] = (red[k, y_next, :, first_cols].astype(f32) + r1[k, 0].astype(f32)).astype(bf16)
        r2_copy(k, 0).start()
        r1_copy(k, 1).wait_recv()
        mid[k, 1] = (red[k, x_next, :, last_cols].astype(f32) + r1[k, 1].astype(f32)).astype(bf16)
        r2_copy(k, 1).start()

    def reduce_in(k):
        for i, cols in enumerate((first_cols, last_cols)):
            total = contrib[k, core, sp, :, cols].astype(f32) + pair2[k, sp, :, cols].astype(f32)
            r1_copy(k, 2 + i).wait_recv()
            r2_copy(k, i).wait_recv()
            total += r1[k, 2 + i].astype(f32) + r2[k, i].astype(f32)

            @pl.when(k < distant)
            def _():
                z2s[k, :, cols] = total.astype(bf16)

            @pl.when(k >= distant)
            def _():
                home[k - distant, :, cols] = total

        @pl.when(k < distant)
        def _():
            z2_copy(k).start()

    normalise(0)
    open_step(distant)
    for d in range(1, nz):
        z1_copy(1, d).start()
    arrive(0)
    open_step(0)
    relay(distant)
    arrive(1)
    open_step(1)
    relay(0)
    for load in loads[12:]:
        load.wait()

    @pl.loop(0, steps + 4)
    def _(k):
        @pl.when(k + 2 < distant)
        def _():
            arrive(k + 2)
            open_step(k + 2)

        @pl.when(k + 1 < distant)
        def _():
            relay(k + 1)

        @pl.when(k == 2)
        def _():
            relay(distant + 1)

        @pl.when(k < steps)
        def _():
            collect(k)

        @pl.when((k >= 2) & (k - 2 < steps))
        def _():
            reduce_out(k - 2)

        @pl.when((k >= 3) & (k - 3 < steps))
        def _():
            reduce_mid(k - 3)

        @pl.when(k >= 4)
        def _():
            reduce_in(k - 4)

        @pl.when(k == 0)
        def _():
            normalise(1)
            open_step(distant + 1)

        @pl.when((k < steps) & (k % 2 == 1))
        def _():
            compute(k // 2)

    for h in range(halves):
        total = mixed[h].astype(f32) + home[h]
        for d in range(1, nz):
            k = step_of(h, d)
            z2_copy(k).wait_recv()
            total += z2[k].astype(f32)
        o_ref[h * band : (h + 1) * band, :] = total.astype(bf16)

    for p in range(1 + heads):
        for i in range(6):
            kv_copy(p, i).wait_send()
    for h in range(halves):
        p1_copy(h).wait_send()
        for d in range(1, nz):
            z1_copy(h, d).wait_send()
            gz_copy(h, d).wait_send()
            z2_copy(step_of(h, d)).wait_send()

    @pl.loop(0, steps)
    def _(k):
        for i in range(6):
            gs_copy(k, i).wait_send()
        for e in range(4):
            gp_copy(k, e).wait_send()
            r1_copy(k, e).wait_send()
        p2_copy(k).wait_send()
        for i in range(2):
            r2_copy(k, i).wait_send()


def per_device(
    n_sp,
    n_tp,
    query_a,
    key_a,
    value_a,
    query_b,
    key_b,
    value_b,
    lambdas,
    gain_a,
    gain_b,
    out_a,
    out_b,
    residual,
    norm_gain,
    route_ids,
    route_weights,
    w_gate,
    w_up,
    w_down,
):
    here, heads, _ = query_a.shape
    da, db = query_a.shape[2] // 2, query_b.shape[2] // 2
    va, vb = value_a.shape[2], value_b.shape[2]
    rows, width = residual.shape
    experts_here, _, hidden = w_gate.shape
    experts_all = experts_here * n_sp
    nz = n_tp // 2
    bf16, f32 = jnp.bfloat16, jnp.float32

    def raw(array):
        pieces = array.shape[2] // 128
        split = array.reshape(here, heads, pieces, 128)
        return split.transpose(0, 2, 1, 3).reshape(here * pieces * heads, 128)

    streams = [raw(a) for a in (query_a, key_a, value_a, query_b, key_b, value_b)]
    lanes = -(-2 * experts_all // 128) * 128
    halves = 2
    band = rows // halves
    steps = halves * nz
    kv_width = 2 * da + va
    assert heads * (2 * db + vb) == kv_width and 2 * db == 128 and vb == 128
    hbm = pl.BlockSpec(memory_space=pl.ANY)
    smem = pl.BlockSpec(memory_space=pltpu.SMEM)
    sem = pltpu.SemaphoreType.DMA
    pairs = [(1 + heads, 6), (halves,), (halves, nz - 1), (halves * (nz - 1),), (steps, 6)]
    pairs += [(steps, 4), (steps,), (steps, 4), (steps, 2), (halves * (nz - 1),)]
    scratch = [pltpu.VMEM(a.shape, bf16) for a in streams]
    scratch += [
        pltpu.VMEM((1, va), f32),
        pltpu.VMEM((1, vb), f32),
        pltpu.VMEM((rows, width), bf16),
        pltpu.VMEM((1, width), f32),
        pltpu.VMEM(out_a.shape, bf16),
        pltpu.VMEM(out_b.shape, bf16),
        pltpu.VMEM(w_gate.shape, bf16),
        pltpu.VMEM(w_up.shape, bf16),
        pltpu.VMEM(w_down.shape, bf16),
        pltpu.VMEM((max(a.shape[0] for a in streams), 128), f32),
        pltpu.VMEM((here, heads * 2 * da), bf16),
        pltpu.VMEM((here, heads * 2 * db), bf16),
        pltpu.VMEM((1 + heads, n_sp, here, kv_width), bf16),
        pltpu.VMEM((here, heads * va), bf16),
        pltpu.VMEM((here, heads * vb), bf16),
        pltpu.VMEM((here, width), f32),
        pltpu.VMEM((rows, lanes), f32),
        pltpu.VMEM((halves, 2, nz, band, width), bf16),
        pltpu.VMEM((halves, nz, band, width), bf16),
        pltpu.VMEM((halves, nz, band, width), bf16),
        pltpu.VMEM((halves, nz - 1, band, width), bf16),
        pltpu.VMEM((halves, band, width), f32),
        pltpu.VMEM((halves, band, width), bf16),
        pltpu.VMEM((steps, n_sp, 2, band, width + lanes), bf16),
        pltpu.VMEM((2 * n_sp * 2 * band, experts_here * hidden), bf16),
        pltpu.VMEM((steps, 2, n_sp, band, width), bf16),
        pltpu.VMEM((steps, n_sp, band, width), bf16),
        pltpu.VMEM((steps, n_sp, band, width), bf16),
        pltpu.VMEM((steps, 4, band, width // 2), bf16),
        pltpu.VMEM((steps, 2, band, width // 2), bf16),
        pltpu.VMEM((steps, 2, band, width // 2), bf16),
        pltpu.VMEM((halves, band, width), f32),
        pltpu.VMEM((halves * (nz - 1), band, width), bf16),
        pltpu.VMEM((halves * (nz - 1), band, width), bf16),
        sem((15,)),
    ]
    for shape in pairs:
        scratch += [sem(shape), sem(shape)]
    return pl.pallas_call(
        functools.partial(layer_kernel, (n_sp, n_tp, heads, da, db, va, vb)),
        out_shape=jax.ShapeDtypeStruct((rows, width), bf16),
        in_specs=[smem] * 3 + [hbm] * 15,
        out_specs=pl.BlockSpec(memory_space=pltpu.VMEM),
        scratch_shapes=scratch,
        compiler_params=pltpu.CompilerParams(
            collective_id=0, has_side_effects=True, vmem_limit_bytes=60 * 1024 * 1024
        ),
    )(
        lambdas,
        route_ids.T,
        route_weights.T,
        *streams,
        gain_a.reshape(1, -1),
        gain_b.reshape(1, -1),
        residual,
        norm_gain.reshape(1, -1),
        out_a,
        out_b,
        w_gate,
        w_up,
        w_down,
    )


def solution(mesh):
    in_specs = (
        P("sp", "tp", None),
        P("sp", "tp", None),
        P("sp", "tp", None),
        P("sp", "tp", None),
        P("sp", "tp", None),
        P("sp", "tp", None),
        P(None, "tp"),
        P(),
        P(),
        P("tp", None),
        P("tp", None),
        P(("sp", "tp"), None),
        P(),
        P(("sp", "tp"), None),
        P(("sp", "tp"), None),
        P("sp", None, "tp"),
        P("sp", None, "tp"),
        P("sp", "tp", None),
    )
    out_specs = P(("sp", "tp"), None)
    n_sp, n_tp = mesh.shape["sp"], mesh.shape["tp"]
    fits = n_sp == 4 and n_tp % 2 == 0 and n_tp <= 8
    body = functools.partial(per_device, n_sp, n_tp) if fits else per_device_plain
    return jax.shard_map(
        body, mesh=mesh, in_specs=in_specs, out_specs=out_specs, check_vma=False
    )
```

```python
import functools

import jax
import jax.numpy as jnp
from jax import lax
from jax.experimental import pallas as pl
from jax.experimental.pallas import tpu as pltpu
from jax.sharding import PartitionSpec as P

EPSILON = 1e-06
LIMIT = 7.0
SLOPE = 1.702
FLOOR = -1e30


def empty_state(heads_here, queries_here, value_width):
    maxima = jnp.full((2, heads_here, queries_here), FLOOR, jnp.float32)
    totals = jnp.zeros((2, heads_here, queries_here), jnp.float32)
    sums = jnp.zeros((2, heads_here, queries_here, value_width), jnp.float32)
    return (maxima, totals, sums)


def absorb_keys(states, queries, keys, values, width):
    maxima, totals, sums = states
    scaling = width ** (-0.5)
    new_maxima = []
    new_totals = []
    new_sums = []
    for which in range(2):
        query_part = queries[:, :, which * width : (which + 1) * width]
        key_part = keys[:, :, which * width : (which + 1) * width]
        scores = (
            jnp.einsum("qhd,khd->hqk", query_part, key_part, preferred_element_type=jnp.float32)
            * scaling
        )
        highest = jnp.maximum(maxima[which], jnp.max(scores, axis=2))
        expo = jnp.exp(scores - highest[:, :, None])
        factor = jnp.exp(maxima[which] - highest)
        new_totals.append(totals[which] * factor + jnp.sum(expo, axis=2))
        carried = jnp.einsum(
            "hqk,khv->hqv", expo.astype(jnp.bfloat16), values, preferred_element_type=jnp.float32
        )
        new_sums.append(sums[which] * factor[:, :, None] + carried)
        new_maxima.append(highest)
    return (jnp.stack(new_maxima), jnp.stack(new_totals), jnp.stack(new_sums))


def finish(states, lambda_row, gain):
    maxima, totals, sums = states
    heard = sums / totals[:, :, :, None]
    differ = heard[0] - lambda_row[:, None, None] * heard[1]
    scaled = lax.rsqrt(jnp.mean(differ * differ, axis=2, keepdims=True) + EPSILON)
    return (differ * scaled * gain).astype(jnp.bfloat16)


def gated_units(grid, w_gate, w_up):
    gate = jnp.einsum("necd,edf->necf", grid, w_gate, preferred_element_type=jnp.float32)
    upward = jnp.einsum("necd,edf->necf", grid, w_up, preferred_element_type=jnp.float32)
    clamped = jnp.minimum(gate, LIMIT)
    return (
        clamped * jax.nn.sigmoid(SLOPE * clamped) * (jnp.clip(upward, -LIMIT, LIMIT) + 1.0)
    ).astype(jnp.bfloat16)


def per_device_plain(
    query_a,
    key_a,
    value_a,
    query_b,
    key_b,
    value_b,
    lambdas,
    gain_a,
    gain_b,
    out_a,
    out_b,
    residual,
    norm_gain,
    route_ids,
    route_weights,
    w_gate,
    w_up,
    w_down,
):
    heads_here = query_a.shape[1]
    queries_here = query_a.shape[0]
    width_a = query_a.shape[2] // 2
    width_b = query_b.shape[2] // 2
    starting = (
        empty_state(heads_here, queries_here, value_a.shape[2]),
        empty_state(heads_here, queries_here, value_b.shape[2]),
    )
    keys_a = lax.all_gather(key_a, "sp", axis=0, tiled=True)
    values_a = lax.all_gather(value_a, "sp", axis=0, tiled=True)
    keys_b = lax.all_gather(key_b, "sp", axis=0, tiled=True)
    values_b = lax.all_gather(value_b, "sp", axis=0, tiled=True)
    state_a = absorb_keys(starting[0], query_a, keys_a, values_a, width_a)
    state_b = absorb_keys(starting[1], query_b, keys_b, values_b, width_b)
    attended_a = finish(state_a, lambdas[0], gain_a)
    attended_b = finish(state_b, lambdas[1], gain_b)
    model_width = out_a.shape[1]
    weights_a = out_a.reshape(heads_here, -1, model_width)
    weights_b = out_b.reshape(heads_here, -1, model_width)
    first = jnp.einsum("hqv,hvd->qd", attended_a, weights_a, preferred_element_type=jnp.float32)
    projected = lax.psum_scatter(
        (
            first
            + jnp.einsum("hqv,hvd->qd", attended_b, weights_b, preferred_element_type=jnp.float32)
        ).astype(jnp.bfloat16),
        "tp",
        scatter_dimension=0,
        tiled=True,
    ).astype(jnp.float32)
    mixed = (residual.astype(jnp.float32) + projected).astype(jnp.bfloat16)
    widened = mixed.astype(jnp.float32)
    normed = (
        widened
        * lax.rsqrt(jnp.mean(widened * widened, axis=1, keepdims=True) + EPSILON)
        * norm_gain
    ).astype(jnp.bfloat16)
    rows_here, chosen = route_ids.shape
    groups = lax.axis_size("sp")
    experts_here = w_gate.shape[0]
    experts_all = experts_here * groups
    capacity = 2 * rows_here * chosen // experts_all
    slots_here = experts_here * capacity
    flat_ids = route_ids.reshape(-1)
    onehot = (flat_ids[:, None] == jnp.arange(experts_all, dtype=jnp.int32)[None, :]).astype(
        jnp.int32
    )
    earlier = jnp.cumsum(onehot, axis=0) - onehot
    target = flat_ids * capacity + jnp.sum(earlier * onehot, axis=1)
    places = jnp.arange(experts_all * capacity, dtype=jnp.int32)
    layout = jnp.any(target.reshape(rows_here, chosen)[None, :, :] == places[:, None, None], axis=2)
    outgoing = jnp.dot(
        layout.astype(jnp.bfloat16), normed, preferred_element_type=jnp.float32
    ).astype(jnp.bfloat16)
    outgoing = outgoing.reshape(groups, slots_here, model_width)
    arrived = lax.all_to_all(outgoing, "sp", split_axis=0, concat_axis=0, tiled=True)
    pieces = lax.all_gather(arrived, "tp", axis=0, tiled=True)
    count = pieces.shape[0]
    grid = pieces.reshape(count, experts_here, capacity, model_width)
    active = gated_units(grid, w_gate, w_up)
    down = jnp.einsum("necf,efd->necd", active, w_down, preferred_element_type=jnp.float32)
    partial_value = down.astype(jnp.bfloat16).reshape(count, slots_here, model_width)
    totals = lax.psum_scatter(
        partial_value.astype(jnp.float32).astype(jnp.bfloat16),
        "tp",
        scatter_dimension=0,
        tiled=True,
    )
    summed = lax.all_to_all(totals, "sp", split_axis=0, concat_axis=0, tiled=True)
    results = summed.reshape(experts_all * capacity, model_width)
    picked = (
        jnp.take(results, target, axis=0)
        .reshape(rows_here, chosen, model_width)
        .astype(jnp.float32)
    )
    combined = jnp.sum(route_weights[:, :, None] * picked, axis=1)
    return (widened + combined).astype(jnp.bfloat16)


PLAN = (
    ("n0 o0 z a1", "o1 f0 f1 a2", "o2 n1 o7 c1", "a3 o3 c0 f2", "f7 a4 o4 c2", "f3 a5 o5 w",),
    ("f4 c3 f5 c7", "a6 o6 r1",),
    ("c5 f6 c4 r2", "r3 m1",),
    ("c6 m2 m3 r5", "r4",),
    ("i2 m5 i1 r6", "m4 i3 i5 m6", "r0 r7 i4 i6", "m0 m7 i0 i7",),
)


def layer_kernel(
    dims,
    lam_ref,
    ids_ref,
    wts_ref,
    qa_hbm,
    ka_hbm,
    va_hbm,
    qb_hbm,
    kb_hbm,
    vb_hbm,
    gain_a_hbm,
    gain_b_hbm,
    res_hbm,
    norm_hbm,
    out_a_hbm,
    out_b_hbm,
    gate_hbm,
    up_hbm,
    down_hbm,
    o_ref,
    qa_raw,
    ka_raw,
    va_raw,
    qb_raw,
    kb_raw,
    vb_raw,
    gain_a,
    gain_b,
    res,
    norm,
    out_a,
    out_b,
    w_gate,
    w_up,
    w_down,
    spread,
    query_a,
    query_b,
    kv_all,
    att_a,
    att_b,
    acc,
    route,
    part,
    pair1,
    sum1,
    z1,
    tot,
    mixed,
    x_all,
    act,
    contrib,
    pair2,
    red,
    r1,
    mid,
    r2,
    home,
    z2s,
    z2,
    loc_sem,
    kv_s,
    kv_r,
    p1_s,
    p1_r,
    z1_s,
    z1_r,
    gz_s,
    gz_r,
    gs_s,
    gs_r,
    gp_s,
    gp_r,
    p2_s,
    p2_r,
    r1_s,
    r1_r,
    r2_s,
    z2_s,
    z2_r,
):
    n_sp, n_tp, heads, da, db, va, vb = dims
    nz = n_tp // 2
    f32, bf16 = jnp.float32, jnp.bfloat16
    sp = lax.axis_index("sp")
    tp = lax.axis_index("tp")
    z, core = tp // 2, tp % 2
    rows, width = res.shape
    halves = part.shape[0]
    band = rows // halves
    steps = halves * nz
    lanes = route.shape[1]
    wide = width + lanes
    cut = -(-wide // 256) * 128
    side = width // 2
    here = query_a.shape[0]
    chunk = 2 * n_sp * 2 * band
    experts_here, _, hidden = w_gate.shape
    experts_all = experts_here * n_sp

    x_next = sp + 1 - 2 * (sp % 2)
    y_next = lax.rem(sp + 2, n_sp)
    corner = n_sp - 1 - sp

    def z_at(d):
        return lax.rem(z + d + nz, nz)

    partner = {"sp": sp, "tp": z * 2 + 1 - core}
    to_x = {"sp": x_next, "tp": tp}
    to_y = {"sp": y_next, "tp": tp}

    def to_z(d):
        return {"sp": sp, "tp": z_at(d) * 2 + core}

    def remote(src, dst, send, recv, device):
        return pltpu.make_async_remote_copy(
            src_ref=src,
            dst_ref=dst,
            send_sem=send,
            recv_sem=recv,
            device_id=device,
            device_id_type=pl.DeviceIdType.MESH,
        )

    def rank(at, owner):
        low = owner - jnp.where(owner > at, 1, 0)
        high = nz - 1 - owner - jnp.where(owner < at, 1, 0)
        return jnp.where(2 * at < nz, low, high)

    def owner_of(r):
        low = r + jnp.where(r >= z, 1, 0)
        high = nz - 1 - r - jnp.where(r >= nz - 1 - z, 1, 0)
        return jnp.where(2 * z < nz, low, high)

    def own_step(h):
        return 0 if h == 0 else h * nz + nz - 1

    def far_steps(h):
        return range(1, nz) if h == 0 else range(h * nz, h * nz + nz - 1)

    def settle(ref, sem):
        pltpu.make_async_copy(ref, ref, sem).wait()

    def kv_copy(p, i):
        owner, target, half = (
            (sp, to_x, 0),
            (sp, to_y, 1),
            (sp, to_x, 1),
            (sp, to_y, 0),
            (x_next, to_y, 0),
            (y_next, to_x, 1),
        )[i]
        size = here // 2
        place = kv_all.at[p, owner, pl.ds(half * size, size)]
        return remote(place, place, kv_s, kv_r.at[p, min(i, 2)], target)

    def p1_copy(h):
        return remote(part.at[h, 1 - core], pair1.at[h], p1_s, p1_r.at[h], partner)

    def z1_copy(h, d):
        return remote(
            sum1.at[h, z_at(d)], z1.at[h, d - 1], z1_s, z1_r.at[h], to_z(d)
        )

    def gz_copy(k, owner, target, send):
        there = far_steps(k // nz)[0] + rank(target, owner)
        return remote(
            x_all.at[k, sp, core],
            x_all.at[there, sp, core],
            gz_s.at[send],
            gz_r.at[there],
            {"sp": sp, "tp": target * 2 + core},
        )

    def spread_z(h, act):
        for i, target in enumerate((z + 1, z - 1)):

            @pl.when((target >= 0) & (target < nz))
            def _():
                act(gz_copy(own_step(h), z, target, halves * nz + 2 * h + i))

    def pass_on(k, act):
        owner = owner_of(k - far_steps(k // nz)[0])
        target = jnp.where(owner < z, z + 1, z - 1)

        @pl.when((target >= 0) & (target < nz))
        def _():
            act(gz_copy(k, owner, target, k))

    def gs_copy(k, i):
        owner, target, half = (
            (sp, to_x, 0),
            (sp, to_y, 1),
            (sp, to_x, 1),
            (sp, to_y, 0),
            (x_next, to_y, 0),
            (y_next, to_x, 1),
        )[i]
        cols = pl.ds(0, cut) if half == 0 else pl.ds(cut, wide - cut)
        place = x_all.at[k, owner, core, :, cols]
        return remote(place, place, gs_s, gs_r.at[k, min(i, 2)], target)

    def gp_copy(k, e):
        block = x_all.at[k, (sp, x_next, y_next, corner)[e], core]
        return remote(block, block, gp_s, gp_r.at[k], partner)

    def p2_copy(k, i):
        cols = pl.ds(i * side, side)
        return remote(
            contrib.at[k, 1 - core, :, :, cols],
            pair2.at[k, :, :, cols],
            p2_s,
            p2_r.at[k, i],
            partner,
        )

    def r1_copy(k, i):
        owner, target, first = (
            (corner, to_x, True),
            (corner, to_y, False),
            (x_next, to_x, True),
            (y_next, to_y, False),
        )[i]
        cols = pl.ds(0, side) if first else pl.ds(side, side)
        return remote(
            red.at[k, owner, :, cols], r1.at[k, i], r1_s, r1_r.at[k, min(i, 2)], target
        )

    def r2_copy(k, i):
        return remote(mid.at[k, i], r2.at[k, i], r2_s, r1_r.at[k, 2], (to_y, to_x)[i])

    def z2_copy(k):
        base = far_steps(k // nz)[0]
        owner = owner_of(k - base)
        there = base + rank(owner, z)
        return remote(
            z2s.at[k], z2.at[there], z2_s, z2_r.at[k // nz], {"sp": sp, "tp": owner * 2 + core}
        )

    moves = (
        (kb_hbm, kb_raw),
        (vb_hbm, vb_raw),
        (ka_hbm, ka_raw),
        (va_hbm, va_raw),
        (qb_hbm, qb_raw),
        (qa_hbm, qa_raw),
        (gain_a_hbm, gain_a),
        (gain_b_hbm, gain_b),
        (out_b_hbm, out_b),
        (out_a_hbm, out_a),
        (res_hbm, res),
        (norm_hbm, norm),
        (gate_hbm, w_gate),
        (up_hbm, w_up),
        (down_hbm, w_down),
    )
    loads = [
        pltpu.make_async_copy(src, dst, loc_sem.at[i]) for i, (src, dst) in enumerate(moves)
    ]
    barrier = pltpu.get_barrier_semaphore()
    greeted = [to_x, to_y, partner] + [to_z(d) for d in range(1, nz)]
    for device in greeted:
        pl.semaphore_signal(
            barrier, inc=1, device_id=device, device_id_type=pl.DeviceIdType.MESH
        )
    for load in loads:
        load.start()

    def deal(raw, out, base, slots):
        count = raw.shape[0]
        spread[:count] = raw[...].astype(f32)
        stride = count // here
        for i in range(stride):
            column = base + slots(i)
            out[:, column : column + 128] = spread[pl.ds(i, here, stride=stride), :].astype(bf16)

    loads[0].wait()
    loads[1].wait()
    own_b = kv_all.at[0, sp]
    deal(kb_raw, own_b, 0, lambda i: i * 128)
    deal(vb_raw, own_b, heads * 2 * db, lambda i: i * 128)
    pl.semaphore_wait(barrier, len(greeted))
    for i in range(4):
        kv_copy(0, i).start()

    def deal_a(raw, base):
        count = raw.shape[0]
        spread[:count] = raw[...].astype(f32)
        stride = count // here
        for i in range(stride):
            c, h = i // heads, i % heads
            column = base + c * 128
            kv_all[1 + h, sp, :, column : column + 128] = spread[
                pl.ds(i, here, stride=stride), :
            ].astype(bf16)

    loads[2].wait()
    deal_a(ka_raw, 0)
    loads[3].wait()
    deal_a(va_raw, 2 * da)
    for i in range(4):
        kv_copy(1, i).start()
    loads[4].wait()
    deal(qb_raw, query_b, 0, lambda i: i * 128)
    loads[5].wait()
    deal(qa_raw, query_a, 0, lambda i: (i % heads) * 2 * da + (i // heads) * 128)
    lane = lax.broadcasted_iota(jnp.int32, (1, lanes), 1)
    folded = jnp.where(lane < experts_all, lane, lane - experts_all)
    for r in range(rows):
        row = jnp.zeros((1, lanes), f32)
        for j in range(ids_ref.shape[0]):
            row += jnp.where(folded == ids_ref[j, r], wts_ref[j, r], 0.0)
        route[r : r + 1, :] = row

    for i in range(2):
        kv_copy(0, i).wait_recv()
        kv_copy(0, 4 + i).start()
    for p in range(2, 1 + heads):
        for i in range(4):
            kv_copy(p, i).start()
    for i in range(2):
        kv_copy(1, i).wait_recv()
        kv_copy(1, 4 + i).start()

    positions = here * n_sp

    def attend(p, q_ref, q0, k0, v0, map_width, value_width, lam, gain):
        heard = []
        for which in range(2):
            if map_width % 128 == 0:
                query = q_ref[:, q0 + which * map_width : q0 + (which + 1) * map_width]
                keys = kv_all[p, :, :, k0 + which * map_width : k0 + (which + 1) * map_width]
            else:
                query = q_ref[:, q0 : q0 + 2 * map_width]
                at = lax.broadcasted_iota(jnp.int32, query.shape, 1)
                inside = (at >= which * map_width) & (at < (which + 1) * map_width)
                query = jnp.where(inside, query.astype(f32), 0.0).astype(bf16)
                keys = kv_all[p, :, :, k0 : k0 + 2 * map_width]
            keys = keys.reshape(positions, keys.shape[2])
            scores = lax.dot_general(
                query, keys, (((1,), (1,)), ((), ())), preferred_element_type=f32
            ) * (map_width**-0.5)
            expo = jnp.exp(scores - jnp.max(scores, axis=1, keepdims=True))
            total = jnp.sum(expo, axis=1, keepdims=True)
            values = kv_all[p, :, :, v0 : v0 + value_width].reshape(positions, value_width)
            carried = jnp.dot(expo.astype(bf16), values, preferred_element_type=f32)
            heard.append(carried / total)
        differ = heard[0] - lam * heard[1]
        scaled = lax.rsqrt(jnp.mean(differ * differ, axis=1, keepdims=True) + EPSILON)
        return (differ * scaled * gain).astype(bf16)

    def attend_a(h):
        att_a[:, h * va : (h + 1) * va] = attend(
            1 + h, query_a, h * 2 * da, 0, 2 * da, da, va, lam_ref[0, h], gain_a[...]
        )

    for load in loads[6:10]:
        load.wait()
    settle(kv_all.at[0, 0:2], kv_r.at[0, 2])
    for h in range(heads):
        att_b[:, h * vb : (h + 1) * vb] = attend(
            0,
            query_b,
            h * 2 * db,
            h * 2 * db,
            heads * 2 * db + h * vb,
            db,
            vb,
            lam_ref[1, h],
            gain_b[...],
        )
    for p in range(2, 1 + heads):
        for i in range(2):
            kv_copy(p, i).wait_recv()
            kv_copy(p, 4 + i).start()
    for h in range(heads - 1):
        settle(kv_all.at[1 + h, 0:2], kv_r.at[1 + h, 2])
        attend_a(h)
    tile, group = 512, 4
    known = (heads - 1) * va

    @pl.loop(0, width // (tile * group))
    def _(i):
        for g in range(group):
            cols = pl.ds(pl.multiple_of((i * group + g) * tile, tile), tile)
            acc[:, cols] = jnp.dot(
                att_a[:, :known], out_a[:known, cols], preferred_element_type=f32
            ) + jnp.dot(att_b[...], out_b[:, cols], preferred_element_type=f32)

    settle(kv_all.at[heads, 0:2], kv_r.at[heads, 2])
    attend_a(heads - 1)

    @pl.loop(0, width // (tile * group))
    def _(i):
        for g in range(group):
            cols = pl.ds(pl.multiple_of((i * group + g) * tile, tile), tile)
            value = acc[:, cols] + jnp.dot(
                att_a[:, known:], out_a[known:, cols], preferred_element_type=f32
            )
            value = value.astype(bf16)
            for zz in range(nz):
                for c in range(2):
                    for h in range(halves):
                        r = (zz * 2 + c) * rows + h * band
                        part[h, c, zz, :, cols] = value[r : r + band]

    for h in range(halves):
        p1_copy(h).start()
    loads[10].wait()
    loads[11].wait()

    def fold(h):
        p1_copy(h).wait_recv()
        for d in range(1, nz):
            zz = z_at(d)
            sum1[h, zz] = (part[h, core, zz].astype(f32) + pair1[h, zz].astype(f32)).astype(bf16)
            if h == 0:
                z1_copy(h, d).start()
        tot[h] = part[h, core, z].astype(f32) + pair1[h, z].astype(f32)

    fold(0)
    fold(1)

    def normalise(h):
        total = tot[h]
        settle(z1.at[h], z1_r.at[h])
        for d in range(1, nz):
            total += z1[h, d - 1].astype(f32)
        here_rows = slice(h * band, (h + 1) * band)
        mix = (res[here_rows].astype(f32) + total).astype(bf16)
        mixed[h] = mix
        full = mix.astype(f32)
        scaled = lax.rsqrt(jnp.mean(full * full, axis=1, keepdims=True) + EPSILON)
        x_all[own_step(h), sp, core, :, :width] = (full * scaled * norm[...]).astype(bf16)
        weights = route[here_rows]
        high = weights.astype(bf16).astype(f32)
        at = lax.broadcasted_iota(jnp.int32, weights.shape, 1)
        x_all[own_step(h), sp, core, :, width:] = jnp.where(
            at < experts_all, high, weights - high
        ).astype(bf16)
        spread_z(h, lambda copy: copy.start())

    def arrive(k):
        block = x_all.at[k, sp, core]
        remote(block, block, gz_s.at[k], gz_r.at[k], to_z(1)).wait_recv()
        pass_on(k, lambda copy: copy.start())

    def open_step(k):
        for i in range(4):
            gs_copy(k, i).start()
        gp_copy(k, 0).start()

    def relay(k):
        for i in range(2):
            gs_copy(k, i).wait_recv()
            gs_copy(k, 4 + i).start()

    def collect(k):
        settle(x_all.at[k, 0:2, 0], gs_r.at[k, 2])
        for e in range(1, 4):
            gp_copy(k, e).start()

    def compute(q):
        for t in range(2):
            settle(x_all.at[2 * q + t, :, 0], gp_r.at[2 * q + t])
        both = pl.ds(2 * q, 2)
        share = x_all[both, :, :, :, width:].reshape(chunk, lanes).astype(f32)
        at = lax.broadcasted_iota(jnp.int32, share.shape, 1)
        x = x_all[both, :, :, :, :width].reshape(chunk, width)
        for j in range(experts_here):
            which = sp * experts_here + j
            weight = jnp.sum(
                jnp.where((at == which) | (at == which + experts_all), share, 0.0),
                axis=1,
                keepdims=True,
            )
            gate = jnp.dot(x, w_gate[j], preferred_element_type=f32)
            upward = jnp.dot(x, w_up[j], preferred_element_type=f32)
            clamped = jnp.minimum(gate, LIMIT)
            active = (
                clamped * jax.nn.sigmoid(SLOPE * clamped) * (jnp.clip(upward, -LIMIT, LIMIT) + 1.0)
            )
            act[:, j * hidden : (j + 1) * hidden] = (active * weight).astype(bf16)
        for i in range(2):
            for g in range(side // tile):
                cols = slice(i * side + g * tile, i * side + (g + 1) * tile)
                rowsum = jnp.zeros((chunk, tile), f32)
                for j in range(experts_here):
                    rowsum += jnp.dot(
                        act[:, j * hidden : (j + 1) * hidden],
                        w_down[j, :, cols],
                        preferred_element_type=f32,
                    )
                value = rowsum.astype(bf16)
                for t in range(2):
                    for s in range(n_sp):
                        for c in range(2):
                            r = ((t * n_sp + s) * 2 + c) * band
                            contrib[2 * q + t, c, s, :, cols] = value[r : r + band]
            for t in range(2):
                p2_copy(2 * q + t, i).start()

    first_cols, last_cols = slice(0, side), slice(side, 2 * side)

    def join(k, s, cols):
        red[k, s, :, cols] = (
            contrib[k, core, s, :, cols].astype(f32) + pair2[k, s, :, cols].astype(f32)
        ).astype(bf16)

    def reduce_out(k):
        p2_copy(k, 0).wait_recv()
        join(k, corner, first_cols)
        r1_copy(k, 0).start()
        join(k, x_next, first_cols)
        p2_copy(k, 1).wait_recv()
        join(k, corner, last_cols)
        r1_copy(k, 1).start()
        r1_copy(k, 2).start()
        join(k, y_next, last_cols)
        r1_copy(k, 3).start()

    def reduce_mid(k):
        join(k, y_next, first_cols)
        join(k, x_next, last_cols)
        r1_copy(k, 0).wait_recv()
        mid[k, 0] = (red[k, y_next, :, first_cols].astype(f32) + r1[k, 0].astype(f32)).astype(bf16)
        r2_copy(k, 0).start()
        r1_copy(k, 1).wait_recv()
        mid[k, 1] = (red[k, x_next, :, last_cols].astype(f32) + r1[k, 1].astype(f32)).astype(bf16)
        r2_copy(k, 1).start()

    def reduce_in(k):
        h, own = k // nz, k == own_step(k // nz)
        settle(r1.at[k], r1_r.at[k, 2])
        for i, cols in enumerate((first_cols, last_cols)):
            total = contrib[k, core, sp, :, cols].astype(f32) + pair2[k, sp, :, cols].astype(f32)
            total += r1[k, 2 + i].astype(f32) + r2[k, i].astype(f32)
            if own:
                home[h, :, cols] = total
            else:
                z2s[k, :, cols] = total.astype(bf16)
        if not own:
            z2_copy(k).start()

    def second_half():
        for d in range(1, nz):
            z1_copy(1, d).start()

    def weights_in():
        for load in loads[12:]:
            load.wait()

    acts = {
        "n": normalise,
        "a": arrive,
        "o": open_step,
        "f": relay,
        "c": collect,
        "r": reduce_out,
        "m": reduce_mid,
        "i": reduce_in,
    }
    def follow(words):
        for word in (word for part in words for word in part.split()):
            if word == "z":
                second_half()
            elif word == "w":
                weights_in()
            else:
                acts[word[0]](int(word[1]))

    @pl.loop(0, steps // 2)
    def _(q):
        for i in range(steps // 2):

            @pl.when(q == i)
            def _():
                follow(PLAN[i])

        compute(q)

    follow(PLAN[-1])

    for h in range(halves):
        total = mixed[h].astype(f32) + home[h]
        settle(z2.at[0 : nz - 1], z2_r.at[h])
        for k in far_steps(h):
            total += z2[k].astype(f32)
        o_ref[h * band : (h + 1) * band, :] = total.astype(bf16)

    settle(kv_all.at[:, 0 : n_sp - 1], kv_s)
    settle(pair1, p1_s)
    settle(z1, z1_s)
    settle(x_all.at[:, 0 : n_sp - 1, 0], gs_s)
    settle(x_all.at[:, :, 0], gp_s)
    settle(pair2, p2_s)
    settle(r1, r1_s)
    settle(r2, r2_s)
    settle(z2.at[0 : halves * (nz - 1)], z2_s)
    for h in range(halves):
        spread_z(h, lambda copy: copy.wait_send())
        for k in far_steps(h):
            pass_on(k, lambda copy: copy.wait_send())


def per_device(
    n_sp,
    n_tp,
    query_a,
    key_a,
    value_a,
    query_b,
    key_b,
    value_b,
    lambdas,
    gain_a,
    gain_b,
    out_a,
    out_b,
    residual,
    norm_gain,
    route_ids,
    route_weights,
    w_gate,
    w_up,
    w_down,
):
    here, heads, _ = query_a.shape
    da, db = query_a.shape[2] // 2, query_b.shape[2] // 2
    va, vb = value_a.shape[2], value_b.shape[2]
    rows, width = residual.shape
    experts_here, _, hidden = w_gate.shape
    experts_all = experts_here * n_sp
    nz = n_tp // 2
    bf16, f32 = jnp.bfloat16, jnp.float32

    def raw(array):
        pieces = array.shape[2] // 128
        split = array.reshape(here, heads, pieces, 128)
        return split.transpose(0, 2, 1, 3).reshape(here * pieces * heads, 128)

    streams = [raw(a) for a in (query_a, key_a, value_a, query_b, key_b, value_b)]
    lanes = -(-2 * experts_all // 128) * 128
    halves = 2
    band = rows // halves
    steps = halves * nz
    kv_width = 2 * da + va
    assert heads * (2 * db + vb) == kv_width and 2 * db == 128 and vb == 128
    hbm = pl.BlockSpec(memory_space=pl.ANY)
    smem = pl.BlockSpec(memory_space=pltpu.SMEM)
    sem = pltpu.SemaphoreType.DMA
    waits = [(), (1 + heads, 3), (), (halves,), (), (halves,), (steps + 2 * halves,), (steps,)]
    waits += [(), (steps, 3), (), (steps,), (), (steps, 2), (), (steps, 3), (), (), (halves,)]
    scratch = [pltpu.VMEM(a.shape, bf16) for a in streams]
    scratch += [
        pltpu.VMEM((1, va), f32),
        pltpu.VMEM((1, vb), f32),
        pltpu.VMEM((rows, width), bf16),
        pltpu.VMEM((1, width), f32),
        pltpu.VMEM(out_a.shape, bf16),
        pltpu.VMEM(out_b.shape, bf16),
        pltpu.VMEM(w_gate.shape, bf16),
        pltpu.VMEM(w_up.shape, bf16),
        pltpu.VMEM(w_down.shape, bf16),
        pltpu.VMEM((max(a.shape[0] for a in streams), 128), f32),
        pltpu.VMEM((here, heads * 2 * da), bf16),
        pltpu.VMEM((here, heads * 2 * db), bf16),
        pltpu.VMEM((1 + heads, n_sp, here, kv_width), bf16),
        pltpu.VMEM((here, heads * va), bf16),
        pltpu.VMEM((here, heads * vb), bf16),
        pltpu.VMEM((here, width), f32),
        pltpu.VMEM((rows, lanes), f32),
        pltpu.VMEM((halves, 2, nz, band, width), bf16),
        pltpu.VMEM((halves, nz, band, width), bf16),
        pltpu.VMEM((halves, nz, band, width), bf16),
        pltpu.VMEM((halves, nz - 1, band, width), bf16),
        pltpu.VMEM((halves, band, width), f32),
        pltpu.VMEM((halves, band, width), bf16),
        pltpu.VMEM((steps, n_sp, 2, band, width + lanes), bf16),
        pltpu.VMEM((2 * n_sp * 2 * band, experts_here * hidden), bf16),
        pltpu.VMEM((steps, 2, n_sp, band, width), bf16),
        pltpu.VMEM((steps, n_sp, band, width), bf16),
        pltpu.VMEM((steps, n_sp, band, width), bf16),
        pltpu.VMEM((steps, 4, band, width // 2), bf16),
        pltpu.VMEM((steps, 2, band, width // 2), bf16),
        pltpu.VMEM((steps, 2, band, width // 2), bf16),
        pltpu.VMEM((halves, band, width), f32),
        pltpu.VMEM((steps, band, width), bf16),
        pltpu.VMEM((steps, band, width), bf16),
        sem((15,)),
    ]
    scratch += [sem(shape) for shape in waits]
    return pl.pallas_call(
        functools.partial(layer_kernel, (n_sp, n_tp, heads, da, db, va, vb)),
        out_shape=jax.ShapeDtypeStruct((rows, width), bf16),
        in_specs=[smem] * 3 + [hbm] * 15,
        out_specs=pl.BlockSpec(memory_space=pltpu.VMEM),
        scratch_shapes=scratch,
        compiler_params=pltpu.CompilerParams(
            collective_id=0, has_side_effects=True, vmem_limit_bytes=60 * 1024 * 1024
        ),
    )(
        lambdas,
        route_ids.T,
        route_weights.T,
        *streams,
        gain_a.reshape(1, -1),
        gain_b.reshape(1, -1),
        residual,
        norm_gain.reshape(1, -1),
        out_a,
        out_b,
        w_gate,
        w_up,
        w_down,
    )


def solution(mesh):
    in_specs = (
        P("sp", "tp", None),
        P("sp", "tp", None),
        P("sp", "tp", None),
        P("sp", "tp", None),
        P("sp", "tp", None),
        P("sp", "tp", None),
        P(None, "tp"),
        P(),
        P(),
        P("tp", None),
        P("tp", None),
        P(("sp", "tp"), None),
        P(),
        P(("sp", "tp"), None),
        P(("sp", "tp"), None),
        P("sp", None, "tp"),
        P("sp", None, "tp"),
        P("sp", "tp", None),
    )
    out_specs = P(("sp", "tp"), None)
    n_sp, n_tp = mesh.shape["sp"], mesh.shape["tp"]
    fits = n_sp == 4 and n_tp % 2 == 0 and n_tp <= 8
    body = functools.partial(per_device, n_sp, n_tp) if fits else per_device_plain
    return jax.shard_map(
        body, mesh=mesh, in_specs=in_specs, out_specs=out_specs, check_vma=False
    )
```

```python
import functools

import jax
import jax.numpy as jnp
from jax import lax
from jax.experimental import pallas as pl
from jax.experimental.pallas import tpu as pltpu
from jax.sharding import PartitionSpec as P

EPSILON = 1e-06
LIMIT = 7.0
SLOPE = 1.702
FLOOR = -1e30


def empty_state(heads_here, queries_here, value_width):
    maxima = jnp.full((2, heads_here, queries_here), FLOOR, jnp.float32)
    totals = jnp.zeros((2, heads_here, queries_here), jnp.float32)
    sums = jnp.zeros((2, heads_here, queries_here, value_width), jnp.float32)
    return (maxima, totals, sums)


def absorb_keys(states, queries, keys, values, width):
    maxima, totals, sums = states
    scaling = width ** (-0.5)
    new_maxima = []
    new_totals = []
    new_sums = []
    for which in range(2):
        query_part = queries[:, :, which * width : (which + 1) * width]
        key_part = keys[:, :, which * width : (which + 1) * width]
        scores = (
            jnp.einsum("qhd,khd->hqk", query_part, key_part, preferred_element_type=jnp.float32)
            * scaling
        )
        highest = jnp.maximum(maxima[which], jnp.max(scores, axis=2))
        expo = jnp.exp(scores - highest[:, :, None])
        factor = jnp.exp(maxima[which] - highest)
        new_totals.append(totals[which] * factor + jnp.sum(expo, axis=2))
        carried = jnp.einsum(
            "hqk,khv->hqv", expo.astype(jnp.bfloat16), values, preferred_element_type=jnp.float32
        )
        new_sums.append(sums[which] * factor[:, :, None] + carried)
        new_maxima.append(highest)
    return (jnp.stack(new_maxima), jnp.stack(new_totals), jnp.stack(new_sums))


def finish(states, lambda_row, gain):
    maxima, totals, sums = states
    heard = sums / totals[:, :, :, None]
    differ = heard[0] - lambda_row[:, None, None] * heard[1]
    scaled = lax.rsqrt(jnp.mean(differ * differ, axis=2, keepdims=True) + EPSILON)
    return (differ * scaled * gain).astype(jnp.bfloat16)


def gated_units(grid, w_gate, w_up):
    gate = jnp.einsum("necd,edf->necf", grid, w_gate, preferred_element_type=jnp.float32)
    upward = jnp.einsum("necd,edf->necf", grid, w_up, preferred_element_type=jnp.float32)
    clamped = jnp.minimum(gate, LIMIT)
    return (
        clamped * jax.nn.sigmoid(SLOPE * clamped) * (jnp.clip(upward, -LIMIT, LIMIT) + 1.0)
    ).astype(jnp.bfloat16)


def per_device_plain(
    query_a,
    key_a,
    value_a,
    query_b,
    key_b,
    value_b,
    lambdas,
    gain_a,
    gain_b,
    out_a,
    out_b,
    residual,
    norm_gain,
    route_ids,
    route_weights,
    w_gate,
    w_up,
    w_down,
):
    heads_here = query_a.shape[1]
    queries_here = query_a.shape[0]
    width_a = query_a.shape[2] // 2
    width_b = query_b.shape[2] // 2
    starting = (
        empty_state(heads_here, queries_here, value_a.shape[2]),
        empty_state(heads_here, queries_here, value_b.shape[2]),
    )
    keys_a = lax.all_gather(key_a, "sp", axis=0, tiled=True)
    values_a = lax.all_gather(value_a, "sp", axis=0, tiled=True)
    keys_b = lax.all_gather(key_b, "sp", axis=0, tiled=True)
    values_b = lax.all_gather(value_b, "sp", axis=0, tiled=True)
    state_a = absorb_keys(starting[0], query_a, keys_a, values_a, width_a)
    state_b = absorb_keys(starting[1], query_b, keys_b, values_b, width_b)
    attended_a = finish(state_a, lambdas[0], gain_a)
    attended_b = finish(state_b, lambdas[1], gain_b)
    model_width = out_a.shape[1]
    weights_a = out_a.reshape(heads_here, -1, model_width)
    weights_b = out_b.reshape(heads_here, -1, model_width)
    first = jnp.einsum("hqv,hvd->qd", attended_a, weights_a, preferred_element_type=jnp.float32)
    projected = lax.psum_scatter(
        (
            first
            + jnp.einsum("hqv,hvd->qd", attended_b, weights_b, preferred_element_type=jnp.float32)
        ).astype(jnp.bfloat16),
        "tp",
        scatter_dimension=0,
        tiled=True,
    ).astype(jnp.float32)
    mixed = (residual.astype(jnp.float32) + projected).astype(jnp.bfloat16)
    widened = mixed.astype(jnp.float32)
    normed = (
        widened
        * lax.rsqrt(jnp.mean(widened * widened, axis=1, keepdims=True) + EPSILON)
        * norm_gain
    ).astype(jnp.bfloat16)
    rows_here, chosen = route_ids.shape
    groups = lax.axis_size("sp")
    experts_here = w_gate.shape[0]
    experts_all = experts_here * groups
    capacity = 2 * rows_here * chosen // experts_all
    slots_here = experts_here * capacity
    flat_ids = route_ids.reshape(-1)
    onehot = (flat_ids[:, None] == jnp.arange(experts_all, dtype=jnp.int32)[None, :]).astype(
        jnp.int32
    )
    earlier = jnp.cumsum(onehot, axis=0) - onehot
    target = flat_ids * capacity + jnp.sum(earlier * onehot, axis=1)
    places = jnp.arange(experts_all * capacity, dtype=jnp.int32)
    layout = jnp.any(target.reshape(rows_here, chosen)[None, :, :] == places[:, None, None], axis=2)
    outgoing = jnp.dot(
        layout.astype(jnp.bfloat16), normed, preferred_element_type=jnp.float32
    ).astype(jnp.bfloat16)
    outgoing = outgoing.reshape(groups, slots_here, model_width)
    arrived = lax.all_to_all(outgoing, "sp", split_axis=0, concat_axis=0, tiled=True)
    pieces = lax.all_gather(arrived, "tp", axis=0, tiled=True)
    count = pieces.shape[0]
    grid = pieces.reshape(count, experts_here, capacity, model_width)
    active = gated_units(grid, w_gate, w_up)
    down = jnp.einsum("necf,efd->necd", active, w_down, preferred_element_type=jnp.float32)
    partial_value = down.astype(jnp.bfloat16).reshape(count, slots_here, model_width)
    totals = lax.psum_scatter(
        partial_value.astype(jnp.float32).astype(jnp.bfloat16),
        "tp",
        scatter_dimension=0,
        tiled=True,
    )
    summed = lax.all_to_all(totals, "sp", split_axis=0, concat_axis=0, tiled=True)
    results = summed.reshape(experts_all * capacity, model_width)
    picked = (
        jnp.take(results, target, axis=0)
        .reshape(rows_here, chosen, model_width)
        .astype(jnp.float32)
    )
    combined = jnp.sum(route_weights[:, :, None] * picked, axis=1)
    return (widened + combined).astype(jnp.bfloat16)


PLAN = (
    ("n0 o0 z a1", "o1 f0 f1 a2", "o2 n1 o7 c1", "a3 o3 c0 f2", "f7 a4 o4 c2", "f3 a5 o5 w",),
    ("f4 c3 f5 c7", "a6 o6 r1",),
    ("c5 f6 c4 r2", "r3 m1",),
    ("c6 m2 m3 r5", "r4",),
    ("i2 m5 i1 r6", "m4 i3 i5 m6", "r0 r7 i4 i6", "m0 m7 i0 i7",),
)


def layer_kernel(
    dims,
    lam_ref,
    ids_ref,
    wts_ref,
    qa_hbm,
    ka_hbm,
    va_hbm,
    qb_hbm,
    kb_hbm,
    vb_hbm,
    gain_a_hbm,
    gain_b_hbm,
    res_hbm,
    norm_hbm,
    out_a_hbm,
    out_b_hbm,
    gate_hbm,
    up_hbm,
    down_hbm,
    o_ref,
    qa_raw,
    ka_raw,
    va_raw,
    qb_raw,
    kb_raw,
    vb_raw,
    gain_a,
    gain_b,
    res,
    norm,
    out_a,
    out_b,
    w_gate,
    w_up,
    w_down,
    spread,
    query_a,
    query_b,
    kv_all,
    att_a,
    att_b,
    acc,
    route,
    part,
    pair1,
    sum1,
    z1,
    tot,
    mixed,
    x_all,
    act,
    contrib,
    pair2,
    red,
    r1,
    mid,
    r2,
    home,
    z2s,
    z2,
    loc_sem,
    kv_s,
    kv_r,
    p1_s,
    p1_r,
    z1_s,
    z1_r,
    gz_s,
    gz_r,
    gs_s,
    gs_r,
    gp_s,
    gp_r,
    p2_s,
    p2_r,
    r1_s,
    r1_r,
    r2_s,
    z2_s,
    z2_r,
):
    n_sp, n_tp, heads, da, db, va, vb = dims
    nz = n_tp // 2
    f32, bf16 = jnp.float32, jnp.bfloat16
    sp = lax.axis_index("sp")
    tp = lax.axis_index("tp")
    z, core = tp // 2, tp % 2
    rows, width = res.shape
    halves = part.shape[0]
    band = rows // halves
    steps = halves * nz
    lanes = route.shape[1]
    wide = width + lanes
    cut = -(-wide // 256) * 128
    side = width // 2
    here = query_a.shape[0]
    chunk = 2 * n_sp * 2 * band
    experts_here, _, hidden = w_gate.shape
    experts_all = experts_here * n_sp

    x_next = sp + 1 - 2 * (sp % 2)
    y_next = lax.rem(sp + 2, n_sp)
    corner = n_sp - 1 - sp

    def z_at(d):
        return lax.rem(z + d + nz, nz)

    partner = {"sp": sp, "tp": z * 2 + 1 - core}
    to_x = {"sp": x_next, "tp": tp}
    to_y = {"sp": y_next, "tp": tp}

    def to_z(d):
        return {"sp": sp, "tp": z_at(d) * 2 + core}

    def remote(src, dst, send, recv, device):
        return pltpu.make_async_remote_copy(
            src_ref=src,
            dst_ref=dst,
            send_sem=send,
            recv_sem=recv,
            device_id=device,
            device_id_type=pl.DeviceIdType.MESH,
        )

    def rank(at, owner):
        low = owner - jnp.where(owner > at, 1, 0)
        high = nz - 1 - owner - jnp.where(owner < at, 1, 0)
        return jnp.where(2 * at < nz, low, high)

    def owner_of(r):
        low = r + jnp.where(r >= z, 1, 0)
        high = nz - 1 - r - jnp.where(r >= nz - 1 - z, 1, 0)
        return jnp.where(2 * z < nz, low, high)

    def own_step(h):
        return 0 if h == 0 else h * nz + nz - 1

    def far_steps(h):
        return range(1, nz) if h == 0 else range(h * nz, h * nz + nz - 1)

    def settle(ref, sem):
        pltpu.make_async_copy(ref, ref, sem).wait()

    def kv_copy(p, i):
        owner, target, half = (
            (sp, to_x, 0),
            (sp, to_y, 1),
            (sp, to_x, 1),
            (sp, to_y, 0),
            (x_next, to_y, 0),
            (y_next, to_x, 1),
        )[i]
        size = here // 2
        place = kv_all.at[p, owner, pl.ds(half * size, size)]
        return remote(place, place, kv_s, kv_r.at[p, min(i, 2)], target)

    def p1_copy(h, i):
        cols = pl.ds(pl.multiple_of(i * side, side), side)
        return remote(
            part.at[h, 1 - core, :, :, cols], pair1.at[h, :, :, cols], p1_s, p1_r.at[h], partner
        )

    def z1_copy(h, d):
        return remote(
            sum1.at[h, z_at(d)], z1.at[h, d - 1], z1_s, z1_r.at[h], to_z(d)
        )

    def gz_copy(k, owner, target, send):
        there = far_steps(k // nz)[0] + rank(target, owner)
        return remote(
            x_all.at[k, sp, core],
            x_all.at[there, sp, core],
            gz_s.at[send],
            gz_r.at[there],
            {"sp": sp, "tp": target * 2 + core},
        )

    def spread_z(h, act):
        for i, target in enumerate((z + 1, z - 1)):

            @pl.when((target >= 0) & (target < nz))
            def _():
                act(gz_copy(own_step(h), z, target, halves * nz + 2 * h + i))

    def pass_on(k, act):
        owner = owner_of(k - far_steps(k // nz)[0])
        target = jnp.where(owner < z, z + 1, z - 1)

        @pl.when((target >= 0) & (target < nz))
        def _():
            act(gz_copy(k, owner, target, k))

    def gs_copy(k, i):
        owner, target, half = (
            (sp, to_x, 0),
            (sp, to_y, 1),
            (sp, to_x, 1),
            (sp, to_y, 0),
            (x_next, to_y, 0),
            (y_next, to_x, 1),
        )[i]
        cols = pl.ds(0, cut) if half == 0 else pl.ds(cut, wide - cut)
        place = x_all.at[k, owner, core, :, cols]
        return remote(place, place, gs_s, gs_r.at[k, min(i, 2)], target)

    def gp_copy(k, e):
        block = x_all.at[k, (sp, x_next, y_next, corner)[e], core]
        return remote(block, block, gp_s, gp_r.at[k], partner)

    def p2_copy(k, i):
        cols = pl.ds(i * side, side)
        return remote(
            contrib.at[k, 1 - core, :, :, cols],
            pair2.at[k, :, :, cols],
            p2_s,
            p2_r.at[k, i],
            partner,
        )

    def r1_copy(k, i):
        owner, target, first = (
            (corner, to_x, True),
            (corner, to_y, False),
            (x_next, to_x, True),
            (y_next, to_y, False),
        )[i]
        cols = pl.ds(0, side) if first else pl.ds(side, side)
        return remote(
            red.at[k, owner, :, cols], r1.at[k, i], r1_s, r1_r.at[k, min(i, 2)], target
        )

    def r2_copy(k, i):
        return remote(mid.at[k, i], r2.at[k, i], r2_s, r1_r.at[k, 2], (to_y, to_x)[i])

    def z2_copy(k):
        base = far_steps(k // nz)[0]
        owner = owner_of(k - base)
        there = base + rank(owner, z)
        return remote(
            z2s.at[k], z2.at[there], z2_s, z2_r.at[k // nz], {"sp": sp, "tp": owner * 2 + core}
        )

    moves = (
        (kb_hbm, kb_raw),
        (vb_hbm, vb_raw),
        (ka_hbm, ka_raw),
        (va_hbm, va_raw),
        (qb_hbm, qb_raw),
        (qa_hbm, qa_raw),
        (gain_a_hbm, gain_a),
        (gain_b_hbm, gain_b),
        (out_b_hbm, out_b),
        (out_a_hbm, out_a),
        (res_hbm, res),
        (norm_hbm, norm),
        (gate_hbm, w_gate),
        (up_hbm, w_up),
        (down_hbm, w_down),
    )
    loads = [
        pltpu.make_async_copy(src, dst, loc_sem.at[i]) for i, (src, dst) in enumerate(moves)
    ]
    barrier = pltpu.get_barrier_semaphore()
    greeted = [to_x, to_y, partner] + [to_z(d) for d in range(1, nz)]
    for device in greeted:
        pl.semaphore_signal(
            barrier, inc=1, device_id=device, device_id_type=pl.DeviceIdType.MESH
        )
    for load in loads:
        load.start()

    def deal(raw, out, base, slots):
        count = raw.shape[0]
        spread[:count] = raw[...].astype(f32)
        stride = count // here
        for i in range(stride):
            column = base + slots(i)
            out[:, column : column + 128] = spread[pl.ds(i, here, stride=stride), :].astype(bf16)

    loads[0].wait()
    loads[1].wait()
    own_b = kv_all.at[0, sp]
    deal(kb_raw, own_b, 0, lambda i: i * 128)
    deal(vb_raw, own_b, heads * 2 * db, lambda i: i * 128)
    pl.semaphore_wait(barrier, len(greeted))
    for i in range(4):
        kv_copy(0, i).start()

    def deal_a(raw, base):
        count = raw.shape[0]
        spread[:count] = raw[...].astype(f32)
        stride = count // here
        for i in range(stride):
            c, h = i // heads, i % heads
            column = base + c * 128
            kv_all[1 + h, sp, :, column : column + 128] = spread[
                pl.ds(i, here, stride=stride), :
            ].astype(bf16)

    loads[2].wait()
    deal_a(ka_raw, 0)
    loads[3].wait()
    deal_a(va_raw, 2 * da)
    for i in range(4):
        kv_copy(1, i).start()
    loads[4].wait()
    deal(qb_raw, query_b, 0, lambda i: i * 128)
    loads[5].wait()
    deal(qa_raw, query_a, 0, lambda i: (i % heads) * 2 * da + (i // heads) * 128)
    lane = lax.broadcasted_iota(jnp.int32, (1, lanes), 1)
    folded = jnp.where(lane < experts_all, lane, lane - experts_all)
    for r in range(rows):
        row = jnp.zeros((1, lanes), f32)
        for j in range(ids_ref.shape[0]):
            row += jnp.where(folded == ids_ref[j, r], wts_ref[j, r], 0.0)
        route[r : r + 1, :] = row

    for i in range(2):
        kv_copy(0, i).wait_recv()
        kv_copy(0, 4 + i).start()
    for p in range(2, 1 + heads):
        for i in range(4):
            kv_copy(p, i).start()
    for i in range(2):
        kv_copy(1, i).wait_recv()
        kv_copy(1, 4 + i).start()

    positions = here * n_sp

    def attend(p, q_ref, q0, k0, v0, map_width, value_width, lam, gain):
        heard = []
        for which in range(2):
            if map_width % 128 == 0:
                query = q_ref[:, q0 + which * map_width : q0 + (which + 1) * map_width]
                keys = kv_all[p, :, :, k0 + which * map_width : k0 + (which + 1) * map_width]
            else:
                query = q_ref[:, q0 : q0 + 2 * map_width]
                at = lax.broadcasted_iota(jnp.int32, query.shape, 1)
                inside = (at >= which * map_width) & (at < (which + 1) * map_width)
                query = jnp.where(inside, query.astype(f32), 0.0).astype(bf16)
                keys = kv_all[p, :, :, k0 : k0 + 2 * map_width]
            keys = keys.reshape(positions, keys.shape[2])
            scores = lax.dot_general(
                query, keys, (((1,), (1,)), ((), ())), preferred_element_type=f32
            ) * (map_width**-0.5)
            expo = jnp.exp(scores - jnp.max(scores, axis=1, keepdims=True))
            total = jnp.sum(expo, axis=1, keepdims=True)
            values = kv_all[p, :, :, v0 : v0 + value_width].reshape(positions, value_width)
            carried = jnp.dot(expo.astype(bf16), values, preferred_element_type=f32)
            heard.append(carried / total)
        differ = heard[0] - lam * heard[1]
        scaled = lax.rsqrt(jnp.mean(differ * differ, axis=1, keepdims=True) + EPSILON)
        return (differ * scaled * gain).astype(bf16)

    def attend_a(h):
        att_a[:, h * va : (h + 1) * va] = attend(
            1 + h, query_a, h * 2 * da, 0, 2 * da, da, va, lam_ref[0, h], gain_a[...]
        )

    for load in loads[6:10]:
        load.wait()
    settle(kv_all.at[0, 0:2], kv_r.at[0, 2])
    for h in range(heads):
        att_b[:, h * vb : (h + 1) * vb] = attend(
            0,
            query_b,
            h * 2 * db,
            h * 2 * db,
            heads * 2 * db + h * vb,
            db,
            vb,
            lam_ref[1, h],
            gain_b[...],
        )
    for p in range(2, 1 + heads):
        for i in range(2):
            kv_copy(p, i).wait_recv()
            kv_copy(p, 4 + i).start()
    tile = 512

    @pl.loop(0, 2)
    def _(i):
        for g in range(side // tile):
            cols = pl.ds(pl.multiple_of(i * side + g * tile, tile), tile)
            acc[:, cols] = jnp.dot(att_b[...], out_b[:, cols], preferred_element_type=f32)

    for h in range(heads):
        settle(kv_all.at[1 + h, 0:2], kv_r.at[1 + h, 2])
        attend_a(h)

    @pl.loop(0, 2)
    def _(i):
        for g in range(side // tile):
            cols = pl.ds(pl.multiple_of(i * side + g * tile, tile), tile)
            value = acc[:, cols] + jnp.dot(
                att_a[...], out_a[:, cols], preferred_element_type=f32
            )
            value = value.astype(bf16)
            for zz in range(nz):
                for c in range(2):
                    for h in range(halves):
                        r = (zz * 2 + c) * rows + h * band
                        part[h, c, zz, :, cols] = value[r : r + band]
        for h in range(halves):
            p1_copy(h, i).start()

    loads[10].wait()
    loads[11].wait()

    def fold(h):
        settle(pair1.at[h], p1_r.at[h])
        for d in range(1, nz):
            zz = z_at(d)
            sum1[h, zz] = (part[h, core, zz].astype(f32) + pair1[h, zz].astype(f32)).astype(bf16)
            if h == 0:
                z1_copy(h, d).start()
        tot[h] = part[h, core, z].astype(f32) + pair1[h, z].astype(f32)

    fold(0)
    fold(1)

    def normalise(h):
        total = tot[h]
        settle(z1.at[h], z1_r.at[h])
        for d in range(1, nz):
            total += z1[h, d - 1].astype(f32)
        here_rows = slice(h * band, (h + 1) * band)
        mix = (res[here_rows].astype(f32) + total).astype(bf16)
        mixed[h] = mix
        full = mix.astype(f32)
        scaled = lax.rsqrt(jnp.mean(full * full, axis=1, keepdims=True) + EPSILON)
        x_all[own_step(h), sp, core, :, :width] = (full * scaled * norm[...]).astype(bf16)
        weights = route[here_rows]
        high = weights.astype(bf16).astype(f32)
        at = lax.broadcasted_iota(jnp.int32, weights.shape, 1)
        x_all[own_step(h), sp, core, :, width:] = jnp.where(
            at < experts_all, high, weights - high
        ).astype(bf16)
        spread_z(h, lambda copy: copy.start())

    def arrive(k):
        block = x_all.at[k, sp, core]
        remote(block, block, gz_s.at[k], gz_r.at[k], to_z(1)).wait_recv()
        pass_on(k, lambda copy: copy.start())

    def open_step(k):
        for i in range(4):
            gs_copy(k, i).start()
        gp_copy(k, 0).start()

    def relay(k):
        for i in range(2):
            gs_copy(k, i).wait_recv()
            gs_copy(k, 4 + i).start()

    def collect(k):
        settle(x_all.at[k, 0:2, 0], gs_r.at[k, 2])
        for e in range(1, 4):
            gp_copy(k, e).start()

    def compute(q):
        for t in range(2):
            settle(x_all.at[2 * q + t, :, 0], gp_r.at[2 * q + t])
        both = pl.ds(2 * q, 2)
        share = x_all[both, :, :, :, width:].reshape(chunk, lanes).astype(f32)
        at = lax.broadcasted_iota(jnp.int32, share.shape, 1)
        x = x_all[both, :, :, :, :width].reshape(chunk, width)
        for j in range(experts_here):
            which = sp * experts_here + j
            weight = jnp.sum(
                jnp.where((at == which) | (at == which + experts_all), share, 0.0),
                axis=1,
                keepdims=True,
            )
            gate = jnp.dot(x, w_gate[j], preferred_element_type=f32)
            upward = jnp.dot(x, w_up[j], preferred_element_type=f32)
            clamped = jnp.minimum(gate, LIMIT)
            active = (
                clamped * jax.nn.sigmoid(SLOPE * clamped) * (jnp.clip(upward, -LIMIT, LIMIT) + 1.0)
            )
            act[:, j * hidden : (j + 1) * hidden] = (active * weight).astype(bf16)
        for i in range(2):
            for g in range(side // tile):
                cols = slice(i * side + g * tile, i * side + (g + 1) * tile)
                rowsum = jnp.zeros((chunk, tile), f32)
                for j in range(experts_here):
                    rowsum += jnp.dot(
                        act[:, j * hidden : (j + 1) * hidden],
                        w_down[j, :, cols],
                        preferred_element_type=f32,
                    )
                value = rowsum.astype(bf16)
                for t in range(2):
                    for s in range(n_sp):
                        for c in range(2):
                            r = ((t * n_sp + s) * 2 + c) * band
                            contrib[2 * q + t, c, s, :, cols] = value[r : r + band]
            for t in range(2):
                p2_copy(2 * q + t, i).start()

    first_cols, last_cols = slice(0, side), slice(side, 2 * side)

    def join(k, s, cols):
        red[k, s, :, cols] = (
            contrib[k, core, s, :, cols].astype(f32) + pair2[k, s, :, cols].astype(f32)
        ).astype(bf16)

    def reduce_out(k):
        p2_copy(k, 0).wait_recv()
        join(k, corner, first_cols)
        r1_copy(k, 0).start()
        join(k, x_next, first_cols)
        p2_copy(k, 1).wait_recv()
        join(k, corner, last_cols)
        r1_copy(k, 1).start()
        r1_copy(k, 2).start()
        join(k, y_next, last_cols)
        r1_copy(k, 3).start()

    def reduce_mid(k):
        join(k, y_next, first_cols)
        join(k, x_next, last_cols)
        r1_copy(k, 0).wait_recv()
        mid[k, 0] = (red[k, y_next, :, first_cols].astype(f32) + r1[k, 0].astype(f32)).astype(bf16)
        r2_copy(k, 0).start()
        r1_copy(k, 1).wait_recv()
        mid[k, 1] = (red[k, x_next, :, last_cols].astype(f32) + r1[k, 1].astype(f32)).astype(bf16)
        r2_copy(k, 1).start()

    def reduce_in(k):
        h, own = k // nz, k == own_step(k // nz)
        settle(r1.at[k], r1_r.at[k, 2])
        for i, cols in enumerate((first_cols, last_cols)):
            total = contrib[k, core, sp, :, cols].astype(f32) + pair2[k, sp, :, cols].astype(f32)
            total += r1[k, 2 + i].astype(f32) + r2[k, i].astype(f32)
            if own:
                home[h, :, cols] = total
            else:
                z2s[k, :, cols] = total.astype(bf16)
        if not own:
            z2_copy(k).start()

    def second_half():
        for d in range(1, nz):
            z1_copy(1, d).start()

    def weights_in():
        for load in loads[12:]:
            load.wait()

    acts = {
        "n": normalise,
        "a": arrive,
        "o": open_step,
        "f": relay,
        "c": collect,
        "r": reduce_out,
        "m": reduce_mid,
        "i": reduce_in,
    }
    def follow(words):
        for word in (word for part in words for word in part.split()):
            if word == "z":
                second_half()
            elif word == "w":
                weights_in()
            else:
                acts[word[0]](int(word[1]))

    @pl.loop(0, steps // 2)
    def _(q):
        for i in range(steps // 2):

            @pl.when(q == i)
            def _():
                follow(PLAN[i])

        compute(q)

    follow(PLAN[-1])

    for h in range(halves):
        total = mixed[h].astype(f32) + home[h]
        settle(z2.at[0 : nz - 1], z2_r.at[h])
        for k in far_steps(h):
            total += z2[k].astype(f32)
        o_ref[h * band : (h + 1) * band, :] = total.astype(bf16)

    settle(kv_all.at[:, 0 : n_sp - 1], kv_s)
    settle(pair1, p1_s)
    settle(z1, z1_s)
    settle(x_all.at[:, 0 : n_sp - 1, 0], gs_s)
    settle(x_all.at[:, :, 0], gp_s)
    settle(pair2, p2_s)
    settle(r1, r1_s)
    settle(r2, r2_s)
    settle(z2.at[0 : halves * (nz - 1)], z2_s)
    for h in range(halves):
        spread_z(h, lambda copy: copy.wait_send())
        for k in far_steps(h):
            pass_on(k, lambda copy: copy.wait_send())


def per_device(
    n_sp,
    n_tp,
    query_a,
    key_a,
    value_a,
    query_b,
    key_b,
    value_b,
    lambdas,
    gain_a,
    gain_b,
    out_a,
    out_b,
    residual,
    norm_gain,
    route_ids,
    route_weights,
    w_gate,
    w_up,
    w_down,
):
    here, heads, _ = query_a.shape
    da, db = query_a.shape[2] // 2, query_b.shape[2] // 2
    va, vb = value_a.shape[2], value_b.shape[2]
    rows, width = residual.shape
    experts_here, _, hidden = w_gate.shape
    experts_all = experts_here * n_sp
    nz = n_tp // 2
    bf16, f32 = jnp.bfloat16, jnp.float32

    def raw(array):
        pieces = array.shape[2] // 128
        split = array.reshape(here, heads, pieces, 128)
        return split.transpose(0, 2, 1, 3).reshape(here * pieces * heads, 128)

    streams = [raw(a) for a in (query_a, key_a, value_a, query_b, key_b, value_b)]
    lanes = -(-2 * experts_all // 128) * 128
    halves = 2
    band = rows // halves
    steps = halves * nz
    kv_width = 2 * da + va
    assert heads * (2 * db + vb) == kv_width and 2 * db == 128 and vb == 128
    hbm = pl.BlockSpec(memory_space=pl.ANY)
    smem = pl.BlockSpec(memory_space=pltpu.SMEM)
    sem = pltpu.SemaphoreType.DMA
    waits = [(), (1 + heads, 3), (), (halves,), (), (halves,), (steps + 2 * halves,), (steps,)]
    waits += [(), (steps, 3), (), (steps,), (), (steps, 2), (), (steps, 3), (), (), (halves,)]
    scratch = [pltpu.VMEM(a.shape, bf16) for a in streams]
    scratch += [
        pltpu.VMEM((1, va), f32),
        pltpu.VMEM((1, vb), f32),
        pltpu.VMEM((rows, width), bf16),
        pltpu.VMEM((1, width), f32),
        pltpu.VMEM(out_a.shape, bf16),
        pltpu.VMEM(out_b.shape, bf16),
        pltpu.VMEM(w_gate.shape, bf16),
        pltpu.VMEM(w_up.shape, bf16),
        pltpu.VMEM(w_down.shape, bf16),
        pltpu.VMEM((max(a.shape[0] for a in streams), 128), f32),
        pltpu.VMEM((here, heads * 2 * da), bf16),
        pltpu.VMEM((here, heads * 2 * db), bf16),
        pltpu.VMEM((1 + heads, n_sp, here, kv_width), bf16),
        pltpu.VMEM((here, heads * va), bf16),
        pltpu.VMEM((here, heads * vb), bf16),
        pltpu.VMEM((here, width), f32),
        pltpu.VMEM((rows, lanes), f32),
        pltpu.VMEM((halves, 2, nz, band, width), bf16),
        pltpu.VMEM((halves, nz, band, width), bf16),
        pltpu.VMEM((halves, nz, band, width), bf16),
        pltpu.VMEM((halves, nz - 1, band, width), bf16),
        pltpu.VMEM((halves, band, width), f32),
        pltpu.VMEM((halves, band, width), bf16),
        pltpu.VMEM((steps, n_sp, 2, band, width + lanes), bf16),
        pltpu.VMEM((2 * n_sp * 2 * band, experts_here * hidden), bf16),
        pltpu.VMEM((steps, 2, n_sp, band, width), bf16),
        pltpu.VMEM((steps, n_sp, band, width), bf16),
        pltpu.VMEM((steps, n_sp, band, width), bf16),
        pltpu.VMEM((steps, 4, band, width // 2), bf16),
        pltpu.VMEM((steps, 2, band, width // 2), bf16),
        pltpu.VMEM((steps, 2, band, width // 2), bf16),
        pltpu.VMEM((halves, band, width), f32),
        pltpu.VMEM((steps, band, width), bf16),
        pltpu.VMEM((steps, band, width), bf16),
        sem((15,)),
    ]
    scratch += [sem(shape) for shape in waits]
    return pl.pallas_call(
        functools.partial(layer_kernel, (n_sp, n_tp, heads, da, db, va, vb)),
        out_shape=jax.ShapeDtypeStruct((rows, width), bf16),
        in_specs=[smem] * 3 + [hbm] * 15,
        out_specs=pl.BlockSpec(memory_space=pltpu.VMEM),
        scratch_shapes=scratch,
        compiler_params=pltpu.CompilerParams(
            collective_id=0, has_side_effects=True, vmem_limit_bytes=60 * 1024 * 1024
        ),
    )(
        lambdas,
        route_ids.T,
        route_weights.T,
        *streams,
        gain_a.reshape(1, -1),
        gain_b.reshape(1, -1),
        residual,
        norm_gain.reshape(1, -1),
        out_a,
        out_b,
        w_gate,
        w_up,
        w_down,
    )


def solution(mesh):
    in_specs = (
        P("sp", "tp", None),
        P("sp", "tp", None),
        P("sp", "tp", None),
        P("sp", "tp", None),
        P("sp", "tp", None),
        P("sp", "tp", None),
        P(None, "tp"),
        P(),
        P(),
        P("tp", None),
        P("tp", None),
        P(("sp", "tp"), None),
        P(),
        P(("sp", "tp"), None),
        P(("sp", "tp"), None),
        P("sp", None, "tp"),
        P("sp", None, "tp"),
        P("sp", "tp", None),
    )
    out_specs = P(("sp", "tp"), None)
    n_sp, n_tp = mesh.shape["sp"], mesh.shape["tp"]
    fits = n_sp == 4 and n_tp % 2 == 0 and n_tp <= 8
    body = functools.partial(per_device, n_sp, n_tp) if fits else per_device_plain
    return jax.shard_map(
        body, mesh=mesh, in_specs=in_specs, out_specs=out_specs, check_vma=False
    )
```
